512 devices in a mesh: ep: 32 (over z, x), tp: 16 (over y, core).
Axes of the slice: x: 4, y: 8, z: 8, core: 2. Of those that a mesh axis runs over, the one named last changes fastest.
Arguments:
- x_in: bfloat16 [4096, 12288], P('tp', 'ep'), may hold values from -6 to 6
- z_in: bfloat16 [4096, 12288], P('tp', 'ep'), may hold values from -6 to 6
- dt_raw: float32 [64, 12288], P('tp', 'ep'), may hold values from -6 to 6
- decay_rate: float32 [64], P('tp'), may hold values from 0 to 1, as said below
- b_in: bfloat16 [256, 12288], P(None, 'ep'), may hold values from -6 to 6
- c_in: bfloat16 [256, 12288], P(None, 'ep'), may hold values from -6 to 6
- conv_x: float32 [4096, 4], P('tp'), may hold values from -3 to 3
- conv_b: float32 [256, 4], replicated, may hold values from -3 to 3
- conv_c: float32 [256, 4], replicated, may hold values from -3 to 3
- head_gain: float32 [4096], P('tp'), may hold values from 0.1 to 1.9
- moe_rows: bfloat16 [5120, 2048], P('ep'), may hold values from -6 to 6
- moe_gain: float32 [2048], replicated, may hold values from 0.1 to 1.9
- routes: int32 [5120, 2], P('ep'), may hold values from 0 to 31, all different within a row; in each aligned block of 160 rows (0 to 159, 160 to 319, ...) at most 20 rows name the same one
- route_logit: float32 [5120, 2], P('ep'), may hold values from -6 to 6
- w_gate: bfloat16 [32, 2048, 5120], P('ep', None, 'tp'), may hold values from -0.125 to 0.125
- w_up: bfloat16 [32, 2048, 5120], P('ep', None, 'tp'), may hold values from -0.125 to 0.125
- w_down: bfloat16 [32, 5120, 2048], P('ep', 'tp'), may hold values from -0.078125 to 0.078125
Outputs:
- mixed: bfloat16 [4096, 12288], P('tp', 'ep')
- moe_out: bfloat16 [2048, 5120], P('tp', 'ep')
The draws below stay inside these ranges and needn't reach their ends.
Inputs may be any that keep to these rules, and one draw needn't show every extreme that they name: `routes`: each row names 2 different experts; among the rows of one index of ep no expert is named more than 20 times, a bound that some block reaches. `decay_rate`: positive rates.
All inputs are finite; a program needn't handle non-finite values.
Results may differ from the reference program's by a relative error of at most 0.018.
Values may be sent and summed in bfloat16 or wider, within the bound.
A program may use at most 64 MiB of HBM per device.

```python
import math
import jax
import jax.numpy as jnp
import numpy as np
from jax import lax

D = 2048
HEADS = 64
HEAD_DIM = 64
GROUPS = 2
NSTATE = 128
KCONV = 4
BLOCK = 128
FF = 5120
TOP = 2
L_DEV = 384
MOE_DEV = 160
SEQLEN = 12288
MTOK = 5120
EXPERTS = 32
CAP = 20
N_EP = 32
N_TP = 16


def draw_decay_rate(key, part):
    order_key, slow_key, fast_key = jax.random.split(jax.random.fold_in(key, 11), 3)
    fast_count = HEADS // 2
    is_fast = jax.random.permutation(order_key, HEADS) < fast_count
    slow_rate = jnp.exp(jax.random.uniform(slow_key, (HEADS,), jnp.float32, math.log(0.05 / SEQLEN), math.log(1.0 / SEQLEN)))
    fast_rate = jnp.exp(jax.random.uniform(fast_key, (HEADS,), jnp.float32, math.log(0.012), math.log(0.04)))
    return jnp.where(is_fast, fast_rate, slow_rate)


def draw_dt_raw(key, part):
    noise_key, span_key, block_key = jax.random.split(jax.random.fold_in(key, 23), 3)
    noise = jnp.clip(0.7 * jax.random.normal(noise_key, (HEADS, SEQLEN), jnp.float32), -4.0, 4.0)
    span_shift = jax.random.uniform(span_key, (HEADS, SEQLEN // L_DEV), jnp.float32, -1.5, 1.5)
    block_shift = jax.random.uniform(block_key, (HEADS, SEQLEN // BLOCK), jnp.float32, -0.5, 0.5)
    return noise + jnp.repeat(span_shift, L_DEV, axis=1) + jnp.repeat(block_shift, BLOCK, axis=1)


def levels(stream_key, extent, pieces, smallest, largest):
    loudness, own = 1.0, jax.random.fold_in(stream_key, 6)
    for axis_at, shards_of in pieces:
        steps = jnp.exp(jax.random.uniform(jax.random.fold_in(own, axis_at), (shards_of,), jnp.float32, smallest / len(pieces), largest / len(pieces)))
        loudness = loudness * jnp.repeat(steps, extent[axis_at] // shards_of).reshape([-1 if axis == axis_at else 1 for axis in range(len(extent))])
    return loudness


def assign_block(stream_key, own, number, rows, amount, top, bound, lean):
    ranking = jax.random.permutation(stream_key, amount)
    crowded, usual = portions_of(amount, rows * top, bound, lean, True), portions_of(amount, rows * top, bound, lean, False)
    places = jnp.arange(amount)

    def named(sizes, rotation):
        used = int((sizes > 0).sum())
        fixed = max(1, used // 4)
        moved = fixed + (places - fixed + rotation * (used - fixed)) % max(1, amount - fixed)
        return jnp.zeros((amount,), jnp.int32).at[ranking[jnp.where(places < fixed, places, moved)]].set(jnp.asarray(sizes, jnp.int32))

    sizes = jnp.where(number % 4 == 0, named(crowded, number // 4), named(usual, number - number // 4 - 1))
    mixed = jax.random.permutation(jax.random.fold_in(own, 3), amount)
    giver, receiver = mixed[0:amount // 2 * 2:2], mixed[1:amount // 2 * 2:2]
    slack = jnp.minimum(sizes[giver] - 1, bound - sizes[receiver]) // 2
    slack = jnp.where((giver == ranking[0]) | (receiver == ranking[0]) | (sizes[receiver] == 0), 0, jnp.maximum(slack, 0))
    moved = jax.random.randint(jax.random.fold_in(own, 4), (amount // 2,), 0, 1 << 20) % (slack + 1)
    sizes = sizes.at[giver].add(-moved).at[receiver].add(moved)
    items = jnp.searchsorted(jnp.cumsum(sizes), jnp.arange(rows * top), side="right").astype(jnp.int32)
    grid = items.reshape(top, rows).T
    grid = grid[jax.random.permutation(jax.random.fold_in(own, 1), rows)]
    rotation = jax.random.randint(jax.random.fold_in(own, 2), (rows, 1), 0, top)
    return jnp.take_along_axis(grid, (jnp.arange(top)[None, :] + rotation) % top, axis=1)


def portions_of(amount, total, most, skew, full):
    loads = [(1 << 20) // math.isqrt(grade ** skew) + 1 for grade in range(1, amount + 1)]
    largest = most if full else min(most, max(-(-total // amount), total * loads[0] // sum(loads)))
    least = 1 if total - largest >= amount - 1 else 0
    given, spare = [largest] + [least] * (amount - 1), total - largest - least * (amount - 1)
    while spare > 0:
        free = [i for i in range(1, amount) if given[i] < largest] or [i for i in range(1, amount) if given[i] < most]
        mass, left = sum([loads[i] for i in free]), spare
        for i in free:
            addition = min(most - given[i], max(1, left * loads[i] // mass), spare)
            given[i] = given[i] + addition
            spare = spare - addition
    return np.array(given)


def gaussian(own_key, dims, width, reach, shards=(), held_as=jnp.bfloat16):
    values = width * jax.random.normal(own_key, dims, jnp.float32)
    if shards:
        values = values * levels(own_key, dims, shards, -0.22, 0.18)
    return jnp.clip(values, -reach, reach).astype(held_as)


def setup_inputs(seed: int = 0) -> dict:
    key_of = jax.random.split(jax.random.key(seed), 18)
    x_in = gaussian(key_of[0], (HEADS * HEAD_DIM, SEQLEN), 1.0, 6.0, ((0, 16), (1, 32)))
    z_in = gaussian(key_of[1], (HEADS * HEAD_DIM, SEQLEN), 1.0, 6.0, ((0, 16), (1, 32)))
    dt_raw = draw_dt_raw(jax.random.fold_in(key_of[17], 71), 0)
    decay_rate = draw_decay_rate(jax.random.fold_in(key_of[17], 71), 0)
    b_in = gaussian(key_of[4], (GROUPS * NSTATE, SEQLEN), 1.0, 6.0, ((1, 32),))
    c_in = gaussian(key_of[5], (GROUPS * NSTATE, SEQLEN), 1.0, 6.0, ((1, 32),))
    conv_x = gaussian(key_of[6], (HEADS * HEAD_DIM, KCONV), KCONV ** -0.5, 3.0, ((0, 16),), jnp.float32)
    conv_b = gaussian(key_of[7], (GROUPS * NSTATE, KCONV), KCONV ** -0.5, 3.0, (), jnp.float32)
    conv_c = gaussian(key_of[8], (GROUPS * NSTATE, KCONV), KCONV ** -0.5, 3.0, (), jnp.float32)
    head_gain = jnp.clip(1.0 + 0.18 * jax.random.normal(key_of[9], (HEADS * HEAD_DIM,), jnp.float32), 0.1, 1.9)
    moe_rows = gaussian(key_of[10], (MTOK, D), 1.0, 6.0, ((0, 32),))
    moe_gain = jnp.clip(1.0 + 0.18 * jax.random.normal(key_of[11], (D,), jnp.float32), 0.1, 1.9)
    routes_keys = jax.random.split(jax.random.fold_in(key_of[12], 1), MTOK // MOE_DEV)
    routes_turns = jax.random.permutation(jax.random.fold_in(key_of[12], 3), MTOK // MOE_DEV)
    routes = jax.vmap(lambda own, number: assign_block(jax.random.fold_in(key_of[12], 2), own, number, MOE_DEV, EXPERTS, TOP, CAP, 2))(routes_keys, routes_turns).reshape((MTOK, TOP))
    route_logit = gaussian(key_of[13], (MTOK, TOP), 1.5, 6.0, ((0, 32),), jnp.float32)
    w_gate = gaussian(key_of[14], (EXPERTS, D, FF), D ** -0.5, 0.125, ((0, 32), (2, 16)))
    w_up = gaussian(key_of[15], (EXPERTS, D, FF), D ** -0.5, 0.125, ((0, 32), (2, 16)))
    w_down = gaussian(key_of[16], (EXPERTS, FF, D), FF ** -0.5, 0.078125, ((0, 32), (1, 16)))
    return dict(x_in=x_in, z_in=z_in, dt_raw=dt_raw, decay_rate=decay_rate, b_in=b_in, c_in=c_in, conv_x=conv_x, conv_b=conv_b, conv_c=conv_c, head_gain=head_gain, moe_rows=moe_rows, moe_gain=moe_gain, routes=routes, route_logit=route_logit, w_gate=w_gate, w_up=w_up, w_down=w_down)


HIGHEST = lax.Precision.HIGHEST
ROW_EPS = 0.1
HEAD_EPS = 1.0

def causal_conv(signal, weight):
    taps = weight.shape[1]
    length = signal.shape[1]
    padded = jnp.pad(signal, ((0, 0), (taps - 1, 0)))
    running = jnp.zeros(signal.shape, jnp.float32)
    for offset in range(taps):
        running = running + weight[:, offset:offset + 1] * padded[:, offset:offset + length]
    return jax.nn.silu(running)

def block_step(state_in, x_block, b_block, c_block, log_block, step_block):
    cum_log = jnp.cumsum(log_block, axis=1)
    seg_log = cum_log[:, :, None] - cum_log[:, None, :]
    causal = jnp.tril(jnp.ones((log_block.shape[1], log_block.shape[1]), bool))
    decay_mask = jnp.exp(jnp.where(causal[None], seg_log, -jnp.inf))
    scores = jnp.einsum('hnt,hns->hts', c_block, b_block, precision=HIGHEST) * decay_mask * step_block[:, None, :]
    inner_term = jnp.einsum('hts,hps->hpt', scores, x_block, precision=HIGHEST)
    carried = jnp.einsum('hnt,hpn->hpt', c_block, state_in, precision=HIGHEST) * jnp.exp(cum_log)[:, None, :]
    tail_weight = jnp.exp(cum_log[:, -1:] - cum_log) * step_block
    fresh_state = jnp.einsum('hps,hns->hpn', x_block * tail_weight[:, None, :], b_block, precision=HIGHEST)
    new_state = jnp.exp(cum_log[:, -1])[:, None, None] * state_in + fresh_state
    return (new_state, inner_term + carried)

def mixer_half(x_in, z_in, dt_raw, decay_rate, b_in, c_in, conv_x, conv_b, conv_c, head_gain):
    x_conv = causal_conv(x_in.astype(jnp.float32), conv_x.astype(jnp.float32)).reshape(HEADS, HEAD_DIM, SEQLEN)
    b_conv = causal_conv(b_in.astype(jnp.float32), conv_b.astype(jnp.float32)).reshape(GROUPS, NSTATE, SEQLEN)
    c_conv = causal_conv(c_in.astype(jnp.float32), conv_c.astype(jnp.float32)).reshape(GROUPS, NSTATE, SEQLEN)
    step_dt = jax.nn.softplus(dt_raw.astype(jnp.float32))
    log_decay = -step_dt * decay_rate.astype(jnp.float32)[:, None]
    block_count = SEQLEN // BLOCK
    per_group = HEADS // GROUPS

    def blocks(tensor):
        return jnp.moveaxis(tensor.reshape(tensor.shape[:-1] + (block_count, BLOCK)), -2, 0)

    def advance(state_in, inputs):
        x_block, b_block, c_block, log_block, step_block = inputs
        return block_step(state_in, x_block, jnp.repeat(b_block, per_group, axis=0), jnp.repeat(c_block, per_group, axis=0), log_block, step_block)
    init_state = jnp.zeros((HEADS, HEAD_DIM, NSTATE), jnp.float32)
    _, block_out = lax.scan(advance, init_state, (blocks(x_conv), blocks(b_conv), blocks(c_conv), blocks(log_decay), blocks(step_dt)))
    y_mixed = jnp.moveaxis(block_out, 0, -2).reshape(HEADS, HEAD_DIM, SEQLEN)
    gated_out = y_mixed * jax.nn.silu(z_in.astype(jnp.float32).reshape(HEADS, HEAD_DIM, SEQLEN))
    head_scale = lax.rsqrt(lax.optimization_barrier(jnp.mean(gated_out * gated_out, axis=1, keepdims=True)) + HEAD_EPS)
    normed_out = gated_out * head_scale * head_gain.astype(jnp.float32).reshape(HEADS, HEAD_DIM, 1)
    return normed_out.reshape(HEADS * HEAD_DIM, SEQLEN).astype(jnp.bfloat16)

def experts_half(moe_rows, moe_gain, routes, route_logit, w_gate, w_up, w_down):
    rows_float = moe_rows.astype(jnp.float32)
    row_scale = lax.rsqrt(lax.optimization_barrier(jnp.mean(rows_float * rows_float, axis=1, keepdims=True)) + ROW_EPS)
    normed = (rows_float * row_scale * moe_gain.astype(jnp.float32)).astype(jnp.bfloat16)
    by_source = routes.reshape(N_EP, MOE_DEV * TOP)
    hit_table = (by_source[:, :, None] == jnp.arange(EXPERTS, dtype=jnp.int32)).astype(jnp.int32)
    slot_rank = lax.optimization_barrier(jnp.sum((jnp.cumsum(hit_table, axis=1) - hit_table) * hit_table, axis=2))
    slot_index = (jnp.arange(N_EP, dtype=jnp.int32)[:, None] * CAP + slot_rank).reshape(-1).astype(jnp.int32)
    expert_index = routes.reshape(-1).astype(jnp.int32)
    token_index = (jnp.arange(MTOK * TOP, dtype=jnp.int32) // TOP).astype(jnp.int32)
    buffer = jnp.zeros((EXPERTS, N_EP * CAP, D), jnp.bfloat16).at[expert_index, slot_index].set(normed[token_index])
    block_width = FF // N_TP

    def run_expert(inputs):
        rows_in, gate_weight, up_weight, down_weight = inputs
        gate_act = jnp.dot(rows_in, gate_weight, preferred_element_type=jnp.float32)
        up_act = jnp.dot(rows_in, up_weight, preferred_element_type=jnp.float32)
        hidden = (jax.nn.silu(gate_act) * up_act).astype(jnp.bfloat16)
        running = jnp.zeros((rows_in.shape[0], D), jnp.float32)
        for part_index in range(N_TP):
            lower = part_index * block_width
            piece_sum = jnp.dot(hidden[:, lower:lower + block_width], down_weight[lower:lower + block_width], preferred_element_type=jnp.float32)
            running = running + lax.optimization_barrier(piece_sum.astype(jnp.bfloat16)).astype(jnp.float32)
        return running.astype(jnp.bfloat16)
    results = lax.map(run_expert, (buffer, w_gate, w_up, w_down))
    picked = results[expert_index, slot_index].astype(jnp.float32).reshape(MTOK, TOP, D)
    weight = jax.nn.sigmoid(route_logit - route_logit[:, ::-1])
    combined = lax.optimization_barrier(jnp.sum(picked * weight[:, :, None], axis=1))
    return combined.T.astype(jnp.bfloat16)

def reference(x_in, z_in, dt_raw, decay_rate, b_in, c_in, conv_x, conv_b, conv_c, head_gain, moe_rows, moe_gain, routes, route_logit, w_gate, w_up, w_down):
    mixed = mixer_half(x_in, z_in, dt_raw, decay_rate, b_in, c_in, conv_x, conv_b, conv_c, head_gain)
    moe_out = experts_half(moe_rows, moe_gain, routes, route_logit, w_gate, w_up, w_down)
    return (mixed, moe_out)
```

```python
import functools
import jax
import jax.numpy as jnp
from jax import lax
from jax.experimental import pallas as pl
from jax.experimental.pallas import tpu as pltpu
from jax.sharding import PartitionSpec as P

HEADS = 64
HEAD_DIM = 64
GROUPS = 2
NSTATE = 128
BLOCK = 128
ROW_EPS = 0.1
HEAD_EPS = 1.0
LANES = 128
F32 = jnp.float32
BF16 = jnp.bfloat16
ROWX = 4
GROUPED = 8
RIM = 16
PACK = 80
VMEM = pltpu.VMEM
MESH = pl.DeviceIdType.MESH


def vmem_specs(count):
    return [pl.BlockSpec(memory_space=VMEM)] * count


def cost(flops, moved):
    return pl.CostEstimate(flops=flops, bytes_accessed=moved, transcendentals=0)


def dot(a, b, dims, precision=None):
    return lax.dot_general(a, b, (dims, ((), ())), preferred_element_type=F32, precision=precision)


def eye(count):
    row = lax.broadcasted_iota(jnp.int32, (count, count), 0)
    col = lax.broadcasted_iota(jnp.int32, (count, count), 1)
    return jnp.where(row == col, 1.0, 0.0).astype(F32)


def upright(flat):
    return dot(flat, eye(flat.shape[0]), ((0,), (0,)), lax.Precision.HIGHEST)


def silu(v):
    return v / (1.0 + jnp.exp(-v))


def conv_rows(signal, rim, weight):
    taps = weight.shape[1]
    joined = jnp.concatenate([rim.astype(F32), signal.astype(F32)], axis=1)
    running = weight[:, taps - 1 : taps] * joined[:, LANES:]
    for back in range(1, taps):
        moved = pltpu.roll(joined, back, 1)[:, LANES:]
        running = running + weight[:, taps - 1 - back : taps - back] * moved
    return silu(running)


def prefix_decays(dt_ref, rate_ref):
    dt = dt_ref[...]
    step = jnp.maximum(dt, 0.0) + jnp.log1p(jnp.exp(-jnp.abs(dt)))
    rate = jnp.where(eye(dt.shape[0]) > 0.0, rate_ref[...], 0.0)
    log_decay = -step * jnp.sum(rate, axis=1, keepdims=True)
    length = dt.shape[1]
    row = lax.broadcasted_iota(jnp.int32, (length, length), 0)
    col = lax.broadcasted_iota(jnp.int32, (length, length), 1)
    upper = jnp.where(row <= col, 1.0, 0.0).astype(F32)
    lower = jnp.where(row >= col, 1.0, 0.0).astype(F32)
    high = lax.Precision.HIGHEST
    cum = dot(log_decay, upper, ((1,), (0,)), high)
    cum_col = dot(lower, log_decay, ((1,), (1,)), high)
    return step, cum, cum_col


def remote(source, target, send, recv, **where):
    return pltpu.make_async_remote_copy(
        src_ref=source, dst_ref=target, send_sem=send, recv_sem=recv, device_id=where, device_id_type=MESH
    )


def offsets(ep_size):
    deep = ep_size // ROWX
    hops = [(dz, dx) for dz in range(deep) for dx in range(ROWX)]
    return sorted(hops, key=lambda h: min(h[0], deep - h[0]) + min(h[1], ROWX - h[1]))


def layer_kernel(
    rows_hbm, gain_hbm, routes_hbm, logit_hbm, x_hbm, tapx_hbm, b_hbm, tapb_hbm, c_hbm, tapc_hbm,
    dt_hbm, rate_hbm, z_hbm, hgain_hbm, gate_hbm, up_hbm, down_hbm,
    mixed_ref, moe_ref,
    rows_ref, gain_ref, routes_ref, logit_ref, x_ref, tapx_ref, b_ref, tapb_ref, c_ref, tapc_ref,
    dt_ref, rate_ref, z_ref, hgain_ref, gu_ref, down_ref,
    rank_ref, weight_ref, pick_ref, outbox, landed, shrink_ref, grow_ref, xall, part, sibp, rs_out, rs_in,
    ret_out, returned,
    rim_out, rim_in, xrim, brim, crim, tap_col, tapb_col, tapc_col, gain_col,
    step_ref, cum_ref, col_ref, score_ref, bconv_ref, cconv_ref, xs_ref, y_ref,
    pre1_out, pre1_in, pre2_out, pre2_in, pre3_out, pre3_in, ex_ref, exr_ref,
    in_sem, box_send, box_recv, rim_send, rim_recv, ag_send, ag_recv, sib_send, sib_recv,
    dd_send, dd_recv, rs_send, rs_recv, ret_send, ret_recv, p1_send, p1_recv, p2_send, p2_recv, p3_send, p3_recv,
    *, ep_size, tp_size,
):
    me, lane = lax.axis_index("ep"), lax.axis_index("tp")
    deep, chips = ep_size // ROWX, tp_size // 2
    far = chips // 2
    z, x = me // ROWX, me % ROWX
    chip, core = lane // 2, lane % 2
    tokens, features = rows_ref.shape
    width = features // tp_size
    heads, length = dt_ref.shape
    pad = outbox.shape[1]
    capacity = xall.shape[1] // ep_size
    hops = offsets(ep_size)
    teams = ep_size // GROUPED
    span = GROUPED * capacity
    half = span // 2
    wide = GROUPED * pad

    loads = {}

    def load(name, source, target):
        copy = pltpu.make_async_copy(source, target, in_sem.at[len(loads)])
        copy.start()
        loads[name] = copy

    load("rows", rows_hbm, rows_ref)
    load("routes", routes_hbm, routes_ref)
    load("logit", logit_hbm, logit_ref)
    load("gain", gain_hbm, gain_ref)
    load("x", x_hbm, x_ref)
    load("b", b_hbm, b_ref)
    load("c", c_hbm, c_ref)
    load("tapx", tapx_hbm, tapx_ref)
    load("tapb", tapb_hbm, tapb_ref)
    load("tapc", tapc_hbm, tapc_ref)
    load("dt", dt_hbm, dt_ref)
    load("rate", rate_hbm, rate_ref)
    hidden_units = down_ref.shape[0]
    main = hidden_units // 256 * 256
    rest = hidden_units - main
    load("gate", gate_hbm.at[0, pl.ds(0, main), :], gu_ref.at[pl.ds(0, main), :])
    load("up", up_hbm.at[0, pl.ds(0, main), :], gu_ref.at[pl.ds(main, main), :])
    load("gate2", gate_hbm.at[0, pl.ds(main, rest), :], gu_ref.at[pl.ds(2 * main, rest), :])
    load("up2", up_hbm.at[0, pl.ds(main, rest), :], gu_ref.at[pl.ds(2 * main + rest, rest), :])
    load("down", down_hbm.at[0], down_ref)
    load("z", z_hbm, z_ref)
    load("hgain", hgain_hbm, hgain_ref)

    barrier = pltpu.get_barrier_semaphore()
    for hop in range(1, ep_size):
        pl.semaphore_signal(barrier, 1, device_id={"ep": (me + hop) % ep_size}, device_id_type=MESH)
    around = [((chip + 1) % chips) * 2 + core, ((chip + chips - 1) % chips) * 2 + core]
    sibling = chip * 2 + 1 - core
    for other in around + [sibling]:
        pl.semaphore_signal(barrier, 1, device_id={"tp": other}, device_id_type=MESH)

    for name in ("routes", "logit"):
        loads[name].wait()
    routes = routes_ref[...]
    logit = logit_ref[...]
    first = 1.0 / (1.0 + jnp.exp(logit[1:2] - logit[0:1]))
    second = 1.0 / (1.0 + jnp.exp(logit[0:1] - logit[1:2]))
    number = lax.broadcasted_iota(jnp.int32, (ep_size, tokens), 0)
    in_first = number == routes[0:1]
    in_second = number == routes[1:2]
    hits = jnp.where(in_first, 1.0, 0.0) + jnp.where(in_second, 1.0, 0.0)
    row = lax.broadcasted_iota(jnp.int32, (tokens, tokens), 0)
    col = lax.broadcasted_iota(jnp.int32, (tokens, tokens), 1)
    earlier = jnp.where(row < col, 1.0, 0.0).astype(BF16)
    rank = dot(hits.astype(BF16), earlier, ((1,), (0,)))
    weight_ref[...] = jnp.where(in_first, first, 0.0) + jnp.where(in_second, second, 0.0)
    rank_ref[...] = jnp.where(hits > 0.0, rank, -1.0)
    srow = lax.broadcasted_iota(jnp.int32, (span, wide), 0)
    scol = lax.broadcasted_iota(jnp.int32, (span, wide), 1)
    grow = lax.broadcasted_iota(jnp.int32, (wide, span), 0)
    gcol = lax.broadcasted_iota(jnp.int32, (wide, span), 1)
    shrink = jnp.zeros((span, wide), F32)
    grown = jnp.zeros((wide, span), F32)
    for slot in range(GROUPED):
        low, gap = slot * pad, slot * (pad - capacity)
        shrink = jnp.where((scol - srow == gap) & (scol >= low) & (scol < low + capacity), 1.0, shrink)
        grown = jnp.where((grow - gcol == gap) & (grow >= low) & (grow < low + capacity), 1.0, grown)
    shrink_ref[...] = shrink.astype(BF16)
    grow_ref[...] = grown.astype(BF16)
    for name in ("rows", "gain"):
        loads[name].wait()
    values = rows_ref[...].astype(F32)
    scale = lax.rsqrt(jnp.mean(values * values, axis=1, keepdims=True) + ROW_EPS)
    mine = pl.ds(pl.multiple_of(lane * width, LANES), width)
    normed = (rows_ref[:, mine].astype(F32) * scale * gain_ref[:, mine]).astype(BF16)
    place = lax.broadcasted_iota(jnp.int32, (pad, tokens), 0).astype(F32)

    def ahead(j):
        dz, dx = hops[j]
        return ((z + dz) % deep) * ROWX + (x + dx) % ROWX

    def behind(j):
        dz, dx = hops[j]
        return ((z + deep - dz) % deep) * ROWX + (x + ROWX - dx) % ROWX

    def box(j):
        return remote(outbox.at[j], landed.at[j], box_send.at[j], box_recv.at[j], ep=ahead(j))

    def back(j):
        return remote(ret_out.at[j], returned.at[j], ret_send.at[j], ret_recv.at[j], ep=behind(j))

    def dispatch(team):
        ones = []
        picks = []
        for slot in range(GROUPED):
            expert = ahead(team * GROUPED + slot)
            same = place == rank_ref[pl.ds(expert, 1), :]
            ones.append(jnp.where(same, 1.0, 0.0))
            picks.append(jnp.where(same, weight_ref[pl.ds(expert, 1), :], 0.0))
        pick_ref[team * wide : (team + 1) * wide, :] = jnp.concatenate(picks, axis=0).astype(BF16)
        chosen = dot(jnp.concatenate(ones, axis=0).astype(BF16), normed, ((1,), (0,)))
        for slot in range(GROUPED):
            j = team * GROUPED + slot
            piece = chosen[slot * pad : (slot + 1) * pad].astype(BF16)
            if j:
                outbox[j] = piece
                box(j).start()
            else:
                landed[j] = piece

    def packed(ref, team):
        pieces = [ref[team * GROUPED + slot].astype(F32) for slot in range(GROUPED)]
        return jnp.concatenate(pieces, axis=0).astype(BF16)

    group = pl.ds(pl.multiple_of(lane * heads // (HEADS // GROUPS) * NSTATE, NSTATE), NSTATE)
    value_rows = x_ref.shape[0]
    pickrow = lax.broadcasted_iota(jnp.int32, (RIM, LANES), 0)
    picklane = lax.broadcasted_iota(jnp.int32, (RIM, LANES), 1)
    edge = jnp.where(picklane == pickrow + (LANES - RIM), 1.0, 0.0).astype(BF16)
    end = slice(length - LANES, length)
    rim = remote(rim_out, rim_in, rim_send.at[0], rim_recv.at[0], ep=(me + 1) % ep_size)

    def send_rims():
        for name in ("x", "b", "c"):
            loads[name].wait()

        @pl.when(me + 1 < ep_size)
        def _():
            rim_out[:, :value_rows] = dot(edge, x_ref[:, end], ((1,), (1,))).astype(BF16)
            rim_out[:, value_rows : value_rows + NSTATE] = dot(edge, b_ref[group, end], ((1,), (1,))).astype(BF16)
            rim_out[:, value_rows + NSTATE :] = dot(edge, c_ref[group, end], ((1,), (1,))).astype(BF16)
            rim.start()

    def columns():
        for name in ("tapx", "tapb", "tapc", "dt", "rate", "hgain"):
            loads[name].wait()
        tap_col[...] = upright(tapx_ref[...])
        tapb_col[...] = upright(tapb_ref[...])
        tapc_col[...] = upright(tapc_ref[...])
        top = lax.broadcasted_iota(jnp.int32, (8, LANES), 0) == 0
        flat = jnp.broadcast_to(hgain_ref[...], (8, hgain_ref.shape[1]))
        gain_col[...] = dot(flat, jnp.where(top, 1.0, 0.0), ((0,), (0,)), lax.Precision.HIGHEST)
        step, cum, cum_col = prefix_decays(dt_ref, rate_ref)
        step_ref[...] = step
        cum_ref[...] = cum
        for head in range(heads):
            col_ref[head] = jnp.broadcast_to(cum_col[:, head : head + 1], (length, LANES))

    def open_rims():
        @pl.when(me > 0)
        def _():
            rim.wait_recv()
            xrim[...] = dot(rim_in[:, :value_rows], edge, ((0,), (0,)))
            brim[...] = dot(rim_in[:, value_rows : value_rows + NSTATE], edge, ((0,), (0,)))
            crim[...] = dot(rim_in[:, value_rows + NSTATE :], edge, ((0,), (0,)))

        @pl.when(me == 0)
        def _():
            for ref in (xrim, brim, crim):
                ref[...] = jnp.zeros_like(ref)

    def state_streams():
        b_conv = conv_rows(b_ref[group, :], brim[...], tapb_col[group, :]).astype(BF16)
        c_conv = conv_rows(c_ref[group, :], crim[...], tapc_col[group, :]).astype(BF16)
        bconv_ref[...] = b_conv
        cconv_ref[...] = c_conv
        score_ref[...] = dot(b_conv, c_conv, ((0,), (0,)))

    def split(reach):
        high = reach.astype(BF16).astype(F32)
        at = lax.broadcasted_iota(jnp.int32, (RIM, NSTATE), 0)
        wideness = (RIM, NSTATE)
        low = jnp.broadcast_to(reach - high, wideness)
        return jnp.where(at == 0, jnp.broadcast_to(high, wideness), jnp.where(at == 1, low, 0.0)).astype(BF16)

    def joinup(block):
        block = block.astype(F32)
        return block[0:1] + block[1:2]

    def end_state(head):
        rows = slice(head * HEAD_DIM, (head + 1) * HEAD_DIM)
        value = conv_rows(x_ref[rows, :], xrim[rows, :], tap_col[rows, :])
        own = cum_ref[head : head + 1, :]
        last = own[:, length - 1 :]
        xs = value * step_ref[head : head + 1, :]
        tail = xs * jnp.exp(last - own)
        pre1_out[head, :HEAD_DIM] = dot(tail.astype(BF16), bconv_ref[...], ((1,), (1,))).astype(BF16)
        pre1_out[head, HEAD_DIM:] = split(jnp.broadcast_to(jnp.exp(last), (1, NSTATE)))
        xs_ref[rows, :] = xs.astype(BF16)

    def local_y(head):
        rows = slice(head * HEAD_DIM, (head + 1) * HEAD_DIM)
        own = cum_ref[head : head + 1, :]
        brow = lax.broadcasted_iota(jnp.int32, (BLOCK, BLOCK), 0)
        bcol = lax.broadcasted_iota(jnp.int32, (BLOCK, BLOCK), 1)
        causal = brow <= bcol
        for target in range(length // BLOCK):
            at = slice(target * BLOCK, (target + 1) * BLOCK)
            pieces = []
            for source in range(target + 1):
                of = slice(source * BLOCK, (source + 1) * BLOCK)
                gap = own[:, at] - col_ref[head, of, :]
                if source == target:
                    gap = jnp.where(causal, gap, -jnp.inf)
                pieces.append((score_ref[of, at] * jnp.exp(gap)).astype(BF16))
            mask = pieces[0] if target == 0 else jnp.concatenate(pieces, axis=0)
            y_ref[rows, at] = dot(xs_ref[rows, : (target + 1) * BLOCK], mask, ((1,), (0,)))

    def close(head):
        rows = slice(head * HEAD_DIM, (head + 1) * HEAD_DIM)
        carried = dot(pre3_in[head], cconv_ref[...], ((1,), (0,)))
        y = y_ref[rows, :] + carried * jnp.exp(cum_ref[head : head + 1, :])
        gated = y * silu(z_ref[rows, :].astype(F32))
        norm = lax.rsqrt(jnp.mean(gated * gated, axis=0, keepdims=True) + HEAD_EPS)
        mixed_ref[rows, :] = (gated * norm * gain_col[rows, 0:1]).astype(BF16)

    def pre1(dx):
        head = (x + dx) % ROWX
        return remote(pre1_out.at[head], pre1_in.at[x], p1_send.at[dx], p1_recv.at[dx], ep=z * ROWX + head)

    def pre2(dz):
        return remote(pre2_out, pre2_in.at[z], p2_send.at[dz], p2_recv.at[dz], ep=((z + dz) % deep) * ROWX + x)

    def pre3(dx):
        spot = (x + dx) % ROWX
        return remote(pre3_out.at[spot], pre3_in.at[x], p3_send.at[dx], p3_recv.at[dx], ep=z * ROWX + spot)

    def spread_states():
        for dx in range(1, ROWX):
            pre1(dx).start()
        pre1_in[x] = pre1_out[x]

    def row_totals():
        for dx in range(1, ROWX):
            pre1(dx).wait_recv()
        total = jnp.zeros((HEAD_DIM, NSTATE), F32)
        reach = jnp.ones((1, NSTATE), F32)
        for spot in range(ROWX):
            ex_ref[spot] = total
            exr_ref[spot] = jnp.broadcast_to(reach, exr_ref.shape[1:])
            hold = joinup(pre1_in[spot, HEAD_DIM:])
            total = pre1_in[spot, :HEAD_DIM].astype(F32) + hold * total
            reach = reach * hold
        pre2_out[:HEAD_DIM] = total.astype(BF16)
        pre2_out[HEAD_DIM:] = split(reach)
        for dz in range(1, deep):

            @pl.when(z + dz < deep)
            def _(dz=dz):
                pre2(dz).start()

    def incoming():
        for dz in range(1, deep):

            @pl.when(z >= dz)
            def _(dz=dz):
                pre2(dz).wait_recv()

        prior = jnp.zeros((HEAD_DIM, NSTATE), F32)
        for level in range(deep - 1):
            after = pre2_in[level, :HEAD_DIM].astype(F32) + joinup(pre2_in[level, HEAD_DIM:]) * prior
            prior = jnp.where(level < z, after, prior)
        for spot in range(ROWX):
            pre3_out[spot] = (ex_ref[spot] + exr_ref[spot, 0:1] * prior).astype(BF16)
        for dx in range(1, ROWX):
            pre3(dx).start()
        pre3_in[x] = pre3_out[x]

    def at_rows(team, d, step):
        if step < far - 1:
            return team * span, span
        return team * span + d * half, half

    def ag(d, team, step):
        sign = 1 - 2 * d
        origin = ((chip + chips - sign * step) % chips) * 2 + core
        start, count = at_rows(team, d, step)
        ref = xall.at[origin, pl.ds(start, count), :]
        return remote(ref, ref, ag_send.at[d, team, step], ag_recv.at[d, team, step], tp=around[d])

    def sib(team, d, step):
        sign = 1 - 2 * d
        origin = ((chip + chips - sign * (step + 1)) % chips) * 2 + core
        start, count = at_rows(team, d, step)
        ref = xall.at[origin, pl.ds(start, count), :]
        index = 0 if step < 0 else 1 + d * far + step
        return remote(ref, ref, sib_send.at[team, index], sib_recv.at[team, index], tp=sibling)

    def arrivals():
        return [(0, -1)] + [(d, step) for step in range(far) for d in range(2)]

    def gather_own(team):
        for slot in range(GROUPED):
            if team or slot:
                box(team * GROUPED + slot).wait_recv()
        block = dot(shrink_ref[...], packed(landed, team), ((1,), (0,))).astype(BF16)
        xall[lane, team * span : (team + 1) * span, :] = block
        for d in range(2):
            ag(d, team, 0).start()
        sib(team, 0, -1).start()

    def gather_step(team, step):
        for d in range(2):
            ag(d, team, step).wait_recv()
            if step + 1 < far:
                ag(d, team, step + 1).start()
            sib(team, d, step).start()

    def ffn(team):
        for d, step in arrivals():
            sib(team, d, step).wait_recv()
        rows = slice(team * span, (team + 1) * span)
        tokens_in = jnp.concatenate([xall[i, rows, :] for i in range(tp_size)], axis=1)
        both = dot(tokens_in, gu_ref[...], ((1,), (1,)))
        hidden = (silu(both[:, :main]) * both[:, main : 2 * main]).astype(BF16)
        last = both[:, 2 * main :]
        extra = (silu(last) * pltpu.roll(last, rest, 1)).astype(BF16)[:, :rest]
        out = dot(hidden, down_ref[:main, :], ((1,), (0,))) + dot(extra, down_ref[main:, :], ((1,), (0,)))
        for i in range(tp_size):
            part[team, i % 2, i // 2] = out[:, i * width : (i + 1) * width].astype(BF16)
        for reach in order_of_need:
            cross(team, reach).start()

    order_of_need = [far]
    for away in range(far - 1, 0, -1):
        order_of_need += [away, chips - away]
    order_of_need.append(0)

    def cross(team, reach):
        at = (chip + reach) % chips
        return remote(
            part.at[team, 1 - core, at], sibp.at[team, at], dd_send.at[team, reach], dd_recv.at[team, reach], tp=sibling
        )

    def own_sum(team, reach):
        at = (chip + reach) % chips
        return part[team, core, at].astype(F32) + sibp[team, at].astype(F32)

    def rs(d, team, step):
        start, count = (d * half, half) if step == 0 else (0, span)
        return remote(
            rs_out.at[d, team, step, pl.ds(start, count), :], rs_in.at[d, team, step, pl.ds(start, count), :],
            rs_send.at[d, team, step], rs_recv.at[d, team, step], tp=around[d],
        )

    def scatter_first(team):
        cross(team, far).wait_recv()
        total = own_sum(team, far).astype(BF16)
        for d in range(2):
            cut = slice(d * half, (d + 1) * half)
            rs_out[d, team, 0, cut, :] = total[cut]
            rs(d, team, 0).start()

    def scatter_step(team, step):
        for d in range(2):
            reach = far - step if d == 0 else chips - (far - step)
            cross(team, reach).wait_recv()
            total = own_sum(team, reach)
            rs(d, team, step - 1).wait_recv()
            if step == 1:
                cut = slice(d * half, (d + 1) * half)
                other = slice((1 - d) * half, (2 - d) * half)
                rs_out[d, team, step, other, :] = total[other].astype(BF16)
                rs_out[d, team, step, cut, :] = (total[cut] + rs_in[d, team, 0, cut, :].astype(F32)).astype(BF16)
            else:
                rs_out[d, team, step] = (total + rs_in[d, team, step - 1].astype(F32)).astype(BF16)
            rs(d, team, step).start()

    def scatter_last(team):
        cross(team, 0).wait_recv()
        total = own_sum(team, 0)
        for d in range(2):
            rs(d, team, far - 1).wait_recv()
            total = total + rs_in[d, team, far - 1].astype(F32)
        spread = dot(grow_ref[...], total.astype(BF16), ((1,), (0,)))
        for slot in range(GROUPED):
            j = team * GROUPED + slot
            piece = spread[slot * pad : (slot + 1) * pad].astype(BF16)
            if j:
                ret_out[j] = piece
                back(j).start()
            else:
                returned[j] = piece

    pl.semaphore_wait(barrier, ep_size - 1 + len(around) + 1)
    for team in range(teams):
        dispatch(team)
    send_rims()
    columns()
    for team in range(teams):
        gather_own(team)
    open_rims()
    state_streams()
    for head in range(heads):
        end_state(head)
    spread_states()
    for step in range(far):
        for team in range(teams):
            gather_step(team, step)
        if step == 0:
            row_totals()
            local_y(0)
        elif step == 1:
            incoming()
            local_y(1)
        elif step == 2:
            local_y(2)
            local_y(3)
            for name in ("gate", "up", "gate2", "up2", "down", "z"):
                loads[name].wait()
    for team in range(teams):
        ffn(team)
        if team:
            scatter_first(team - 1)
    scatter_first(teams - 1)
    for step in range(1, far):
        for team in range(teams):
            scatter_step(team, step)
        if step == 1:
            for dx in range(1, ROWX):
                pre3(dx).wait_recv()
            close(0)
        elif step == 2:
            close(1)
            close(2)
        else:
            close(3)
    for team in range(teams):
        scatter_last(team)
    total = jnp.zeros((tokens, width), F32)
    for team in range(teams):
        for slot in range(GROUPED):
            if team or slot:
                back(team * GROUPED + slot).wait_recv()
        total = total + dot(pick_ref[team * wide : (team + 1) * wide, :], packed(returned, team), ((0,), (0,)))
    moe_ref[...] = total.astype(BF16)

    for j in range(1, ep_size):
        box(j).wait_send()
        back(j).wait_send()

    @pl.when(me + 1 < ep_size)
    def _():
        rim.wait_send()

    for dx in range(1, ROWX):
        pre1(dx).wait_send()
        pre3(dx).wait_send()
    for dz in range(1, deep):

        @pl.when(z + dz < deep)
        def _(dz=dz):
            pre2(dz).wait_send()

    for team in range(teams):
        for d in range(2):
            for step in range(far):
                ag(d, team, step).wait_send()
                rs(d, team, step).wait_send()
        for d, step in arrivals():
            sib(team, d, step).wait_send()
        for reach in range(chips):
            cross(team, reach).wait_send()


def on_device(
    x_in, z_in, dt_raw, decay_rate, b_in, c_in, conv_x, conv_b, conv_c, head_gain,
    moe_rows, moe_gain, routes, route_logit, w_gate, w_up, w_down,
):
    heads, length = dt_raw.shape
    value_rows = x_in.shape[0]
    taps = conv_x.shape[1]
    tp_size = lax.axis_size("tp")
    ep_size = lax.axis_size("ep")
    tokens, features = moe_rows.shape
    top = routes.shape[1]
    capacity = 2 * tokens * top // ep_size
    pad = (capacity + 7) // 8 * 8
    width = features // tp_size
    hidden_units = w_gate.shape[2]
    slots = ep_size * capacity
    deep, chips = ep_size // ROWX, tp_size // 2
    far, teams, span = chips // 2, ep_size // GROUPED, GROUPED * capacity
    dma = pltpu.SemaphoreType.DMA
    shape = jax.ShapeDtypeStruct
    groups = b_in.shape[0]

    mixed, moe = pl.pallas_call(
        functools.partial(layer_kernel, ep_size=ep_size, tp_size=tp_size),
        out_shape=(shape((value_rows, length), BF16), shape((tokens, width), BF16)),
        in_specs=[pl.BlockSpec(memory_space=pltpu.HBM)] * 17,
        out_specs=tuple(vmem_specs(2)),
        scratch_shapes=[
            VMEM((tokens, features), BF16), VMEM((1, features), F32), VMEM((top, tokens), jnp.int32), VMEM((top, tokens), F32),
            VMEM((value_rows, length), BF16), VMEM((taps, value_rows), F32),
            VMEM((groups, length), BF16), VMEM((taps, groups), F32), VMEM((groups, length), BF16), VMEM((taps, groups), F32),
            VMEM((heads, length), F32), VMEM((1, heads), F32), VMEM((value_rows, length), BF16), VMEM((1, value_rows), F32),
            VMEM((2 * hidden_units, features), BF16), VMEM((hidden_units, features), BF16),
            VMEM((ep_size, tokens), F32), VMEM((ep_size, tokens), F32), VMEM((ep_size * pad, tokens), BF16),
            VMEM((ep_size, pad, width), BF16), VMEM((ep_size, pad, width), BF16),
            VMEM((span, GROUPED * pad), BF16), VMEM((GROUPED * pad, span), BF16),
            VMEM((tp_size, slots, width), BF16),
            VMEM((teams, 2, chips, span, width), BF16), VMEM((teams, chips, span, width), BF16),
            VMEM((2, teams, far, span, width), BF16), VMEM((2, teams, far, span, width), BF16),
            VMEM((ep_size, pad, width), BF16), VMEM((ep_size, pad, width), BF16),
            VMEM((RIM, value_rows + 2 * NSTATE), BF16), VMEM((RIM, value_rows + 2 * NSTATE), BF16),
            VMEM((value_rows, LANES), F32), VMEM((NSTATE, LANES), F32), VMEM((NSTATE, LANES), F32),
            VMEM((value_rows, taps), F32), VMEM((groups, taps), F32), VMEM((groups, taps), F32),
            VMEM((value_rows, LANES), F32),
            VMEM((heads, length), F32), VMEM((heads, length), F32), VMEM((heads, length, LANES), F32),
            VMEM((length, length), F32), VMEM((NSTATE, length), BF16), VMEM((NSTATE, length), BF16),
            VMEM((value_rows, length), BF16), VMEM((value_rows, length), F32),
            VMEM((heads, PACK, NSTATE), BF16), VMEM((ROWX, PACK, NSTATE), BF16),
            VMEM((PACK, NSTATE), BF16), VMEM((deep, PACK, NSTATE), BF16),
            VMEM((ROWX, HEAD_DIM, NSTATE), BF16), VMEM((ROWX, HEAD_DIM, NSTATE), BF16),
            VMEM((ROWX, HEAD_DIM, NSTATE), F32), VMEM((ROWX, 8, NSTATE), F32),
            dma((19,)), dma((ep_size,)), dma((ep_size,)), dma((1,)), dma((1,)),
            dma((2, teams, far)), dma((2, teams, far)), dma((teams, 1 + 2 * far)), dma((teams, 1 + 2 * far)),
            dma((teams, chips)), dma((teams, chips)), dma((2, teams, far)), dma((2, teams, far)),
            dma((ep_size,)), dma((ep_size,)), dma((ROWX,)), dma((ROWX,)), dma((deep,)), dma((deep,)), dma((ROWX,)), dma((ROWX,)),
        ],
        compiler_params=pltpu.CompilerParams(collective_id=0, has_side_effects=True, vmem_limit_bytes=56 * 2**20),
        name="layer",
    )(
        moe_rows, moe_gain.reshape(1, features), routes.T, route_logit.T,
        x_in, conv_x.T, b_in, conv_b.T, c_in, conv_c.T, dt_raw, decay_rate.reshape(1, heads),
        z_in, head_gain.reshape(1, value_rows),
        jnp.swapaxes(w_gate, 1, 2), jnp.swapaxes(w_up, 1, 2), w_down,
    )
    return (mixed, moe.T)


def solution(mesh):
    return jax.shard_map(
        on_device,
        mesh=mesh,
        in_specs=(
            P("tp", "ep"), P("tp", "ep"), P("tp", "ep"), P("tp"), P(None, "ep"), P(None, "ep"),
            P("tp", None), P(), P(), P("tp"), P("ep", None), P(), P("ep", None), P("ep", None),
            P("ep", None, "tp"), P("ep", None, "tp"), P("ep", "tp", None),
        ),
        out_specs=(P("tp", "ep"), P("tp", "ep")),
        check_vma=False,
    )
```

```python
import functools
import jax
import jax.numpy as jnp
from jax import lax
from jax.experimental import pallas as pl
from jax.experimental.pallas import tpu as pltpu
from jax.sharding import PartitionSpec as P

HEADS = 64
HEAD_DIM = 64
GROUPS = 2
NSTATE = 128
BLOCK = 128
ROW_EPS = 0.1
HEAD_EPS = 1.0
LANES = 128
F32 = jnp.float32
BF16 = jnp.bfloat16
ROWX = 4
GROUPED = 8
RIM = 16
PACK = 80
PLAN = (
    ("columns",), ("decays",), ("turn", 0), ("turn", 1), ("turn", 2), ("turn", 3), ("gather_own", 0), ("open_rims",),
    ("b_stream",), ("c_stream",), ("gather_own", 1), ("end_state", 0), ("end_state", 1), ("end_state", 2),
    ("end_state", 3), ("gather_step", 0, 0), ("scores",), ("spread_states",), ("local_y", 0), ("local_y", 1),
    ("local_y", 2), ("gather_own", 2), ("local_y", 3), ("gather_step", 1, 0), ("gather_own", 3),
    ("gather_step", 0, 1), ("gather_step", 2, 0), ("gather_step", 1, 1), ("gather_step", 3, 0), ("gather_step", 0, 2),
    ("gather_step", 2, 1), ("row_totals",), ("gather_step", 1, 2), ("gather_step", 3, 1), ("gather_step", 0, 3),
    ("gather_step", 2, 2), ("ffn", 0), ("gather_step", 1, 3), ("gather_step", 3, 2), ("gather_step", 2, 3),
    ("ffn", 1), ("gather_step", 3, 3), ("scatter_first", 0), ("ffn", 2), ("ffn", 3), ("scatter_first", 1),
    ("scatter_step", 0, 1), ("incoming",), ("scatter_first", 2), ("scatter_first", 3), ("scatter_step", 1, 1),
    ("scatter_step", 0, 2), ("scatter_step", 2, 1), ("scatter_step", 3, 1), ("scatter_step", 1, 2),
    ("scatter_step", 0, 3), ("close", 0), ("close", 1), ("close", 2), ("scatter_step", 2, 2), ("close", 3),
    ("scatter_step", 3, 2), ("scatter_step", 1, 3), ("scatter_last", 0), ("scatter_step", 2, 3),
    ("scatter_step", 3, 3), ("scatter_last", 1), ("scatter_last", 2), ("scatter_last", 3),
)
VMEM = pltpu.VMEM
MESH = pl.DeviceIdType.MESH


def vmem_specs(count):
    return [pl.BlockSpec(memory_space=VMEM)] * count


def cost(flops, moved):
    return pl.CostEstimate(flops=flops, bytes_accessed=moved, transcendentals=0)


def dot(a, b, dims, precision=None):
    return lax.dot_general(a, b, (dims, ((), ())), preferred_element_type=F32, precision=precision)


def eye(count):
    row = lax.broadcasted_iota(jnp.int32, (count, count), 0)
    col = lax.broadcasted_iota(jnp.int32, (count, count), 1)
    return jnp.where(row == col, 1.0, 0.0).astype(F32)


def upright(flat):
    return dot(flat, eye(flat.shape[0]), ((0,), (0,)), lax.Precision.HIGHEST)


def silu(v):
    return v / (1.0 + jnp.exp(-v))


def conv_rows(signal, rim, weight):
    taps = weight.shape[1]
    joined = jnp.concatenate([rim.astype(F32), signal.astype(F32)], axis=1)
    running = weight[:, taps - 1 : taps] * joined[:, LANES:]
    for back in range(1, taps):
        moved = pltpu.roll(joined, back, 1)[:, LANES:]
        running = running + weight[:, taps - 1 - back : taps - back] * moved
    return silu(running)


def prefix_decays(dt_ref, rate_ref):
    dt = dt_ref[...]
    step = jnp.maximum(dt, 0.0) + jnp.log1p(jnp.exp(-jnp.abs(dt)))
    rate = jnp.where(eye(dt.shape[0]) > 0.0, rate_ref[...], 0.0)
    log_decay = -step * jnp.sum(rate, axis=1, keepdims=True)
    length = dt.shape[1]
    row = lax.broadcasted_iota(jnp.int32, (length, length), 0)
    col = lax.broadcasted_iota(jnp.int32, (length, length), 1)
    upper = jnp.where(row <= col, 1.0, 0.0).astype(F32)
    lower = jnp.where(row >= col, 1.0, 0.0).astype(F32)
    high = lax.Precision.HIGHEST
    cum = dot(log_decay, upper, ((1,), (0,)), high)
    cum_col = dot(lower, log_decay, ((1,), (1,)), high)
    return step, cum, cum_col


def remote(source, target, send, recv, **where):
    return pltpu.make_async_remote_copy(
        src_ref=source, dst_ref=target, send_sem=send, recv_sem=recv, device_id=where, device_id_type=MESH
    )


def offsets(ep_size):
    deep = ep_size // ROWX
    hops = [(dz, dx) for dz in range(deep) for dx in range(ROWX)]
    near = sorted(hops, key=lambda h: min(h[0], deep - h[0]) + min(h[1], ROWX - h[1]))
    first, second = near[:GROUPED], near[GROUPED : 2 * GROUPED]
    return first + near[2 * GROUPED :] + second


def layer_kernel(
    rows_hbm, gain_hbm, routes_hbm, logit_hbm, x_hbm, tapx_hbm, b_hbm, tapb_hbm, c_hbm, tapc_hbm,
    dt_hbm, rate_hbm, z_hbm, hgain_hbm, gate_hbm, up_hbm, down_hbm,
    mixed_ref, moe_ref,
    rows_ref, gain_ref, routes_ref, logit_ref, x_ref, tapx_ref, b_ref, tapb_ref, c_ref, tapc_ref,
    dt_ref, rate_ref, z_ref, hgain_ref, gu_ref, gut_ref, down_ref,
    rank_ref, weight_ref, pick_ref, outbox, landed, xall, part, sibp, rs_out, rs_in,
    ret_out, returned,
    rim_out, rim_in, xrim, brim, crim, tap_col, tapb_col, tapc_col, gain_col,
    step_ref, cum_ref, col_ref, score_ref, bconv_ref, cconv_ref, xs_ref, y_ref,
    pre1_out, pre1_in, pre2_out, pre2_in, pre3_out, pre3_in, ex_ref, exr_ref,
    in_sem, box_send, box_recv, rim_send, rim_recv, ag_send, ag_recv, sib_send, sib_recv,
    dd_send, dd_recv, rs_send, rs_recv, ret_send, ret_recv, p1_send, p1_recv, p2_send, p2_recv, p3_send, p3_recv,
    *, ep_size, tp_size,
):
    me, lane = lax.axis_index("ep"), lax.axis_index("tp")
    deep, chips = ep_size // ROWX, tp_size // 2
    far = chips // 2
    z, x = me // ROWX, me % ROWX
    chip, core = lane // 2, lane % 2
    tokens, features = rows_ref.shape
    width = features // tp_size
    heads, length = dt_ref.shape
    pad = outbox.shape[1]
    capacity = xall.shape[1] // ep_size
    hops = offsets(ep_size)
    teams = ep_size // GROUPED
    span = GROUPED * capacity
    half = span // 2
    wide = GROUPED * pad

    loads = {}

    def load(name, source, target):
        copy = pltpu.make_async_copy(source, target, in_sem.at[len(loads)])
        copy.start()
        loads[name] = copy

    load("rows", rows_hbm, rows_ref)
    load("routes", routes_hbm, routes_ref)
    load("logit", logit_hbm, logit_ref)
    load("gain", gain_hbm, gain_ref)
    load("x", x_hbm, x_ref)
    load("b", b_hbm, b_ref)
    load("c", c_hbm, c_ref)
    load("tapx", tapx_hbm, tapx_ref)
    load("tapb", tapb_hbm, tapb_ref)
    load("tapc", tapc_hbm, tapc_ref)
    load("dt", dt_hbm, dt_ref)
    load("rate", rate_hbm, rate_ref)
    hidden_units = down_ref.shape[0]
    main = hidden_units // 256 * 256
    rest = hidden_units - main
    load("gate", gate_hbm.at[0, pl.ds(0, main), :], gu_ref.at[pl.ds(0, main), :])
    load("up", up_hbm.at[0, pl.ds(0, main), :], gu_ref.at[pl.ds(main, main), :])
    load("gate2", gate_hbm.at[0, pl.ds(main, rest), :], gu_ref.at[pl.ds(2 * main, rest), :])
    load("up2", up_hbm.at[0, pl.ds(main, rest), :], gu_ref.at[pl.ds(2 * main + rest, rest), :])
    load("down", down_hbm.at[0], down_ref)
    load("z", z_hbm, z_ref)
    load("hgain", hgain_hbm, hgain_ref)

    barrier = pltpu.get_barrier_semaphore()
    for hop in range(1, ep_size):
        pl.semaphore_signal(barrier, 1, device_id={"ep": (me + hop) % ep_size}, device_id_type=MESH)
    around = [((chip + 1) % chips) * 2 + core, ((chip + chips - 1) % chips) * 2 + core]
    sibling = chip * 2 + 1 - core
    for other in around + [sibling]:
        pl.semaphore_signal(barrier, 1, device_id={"tp": other}, device_id_type=MESH)

    for name in ("routes", "logit"):
        loads[name].wait()
    routes = routes_ref[...]
    logit = logit_ref[...]
    first = 1.0 / (1.0 + jnp.exp(logit[1:2] - logit[0:1]))
    second = 1.0 / (1.0 + jnp.exp(logit[0:1] - logit[1:2]))
    number = lax.broadcasted_iota(jnp.int32, (ep_size, tokens), 0)
    in_first = number == routes[0:1]
    in_second = number == routes[1:2]
    hits = jnp.where(in_first, 1.0, 0.0) + jnp.where(in_second, 1.0, 0.0)
    row = lax.broadcasted_iota(jnp.int32, (tokens, tokens), 0)
    col = lax.broadcasted_iota(jnp.int32, (tokens, tokens), 1)
    earlier = jnp.where(row < col, 1.0, 0.0).astype(BF16)
    rank = dot(hits.astype(BF16), earlier, ((1,), (0,)))
    weight_ref[...] = jnp.where(in_first, first, 0.0) + jnp.where(in_second, second, 0.0)
    rank_ref[...] = jnp.where(hits > 0.0, rank, -1.0)
    for name in ("rows", "gain"):
        loads[name].wait()
    values = rows_ref[...].astype(F32)
    scale = lax.rsqrt(jnp.mean(values * values, axis=1, keepdims=True) + ROW_EPS)
    mine = pl.ds(pl.multiple_of(lane * width, LANES), width)
    normed = (rows_ref[:, mine].astype(F32) * scale * gain_ref[:, mine]).astype(BF16)
    place = lax.broadcasted_iota(jnp.int32, (pad, tokens), 0).astype(F32)

    def ahead(j):
        dz, dx = hops[j]
        return ((z + dz) % deep) * ROWX + (x + dx) % ROWX

    def behind(j):
        dz, dx = hops[j]
        return ((z + deep - dz) % deep) * ROWX + (x + ROWX - dx) % ROWX

    def box(j):
        return remote(outbox.at[j], landed.at[j], box_send.at[j], box_recv.at[j], ep=ahead(j))

    def back(j):
        return remote(ret_out.at[j], returned.at[j], ret_send.at[j], ret_recv.at[j], ep=behind(j))

    def dispatch(team):
        ones = []
        picks = []
        for slot in range(GROUPED):
            expert = ahead(team * GROUPED + slot)
            same = place == rank_ref[pl.ds(expert, 1), :]
            ones.append(jnp.where(same, 1.0, 0.0))
            picks.append(jnp.where(same, weight_ref[pl.ds(expert, 1), :], 0.0))
        pick_ref[team * wide : (team + 1) * wide, :] = jnp.concatenate(picks, axis=0).astype(BF16)
        chosen = dot(jnp.concatenate(ones, axis=0).astype(BF16), normed, ((1,), (0,)))
        for slot in range(GROUPED):
            j = team * GROUPED + slot
            piece = chosen[slot * pad : (slot + 1) * pad].astype(BF16)
            if j:
                outbox[j] = piece
                box(j).start()
            else:
                landed[j] = piece

    def packed(ref, team):
        pieces = [ref[team * GROUPED + slot].astype(F32) for slot in range(GROUPED)]
        return jnp.concatenate(pieces, axis=0).astype(BF16)

    group = pl.ds(pl.multiple_of(lane * heads // (HEADS // GROUPS) * NSTATE, NSTATE), NSTATE)
    value_rows = x_ref.shape[0]
    pickrow = lax.broadcasted_iota(jnp.int32, (RIM, LANES), 0)
    picklane = lax.broadcasted_iota(jnp.int32, (RIM, LANES), 1)
    edge = jnp.where(picklane == pickrow + (LANES - RIM), 1.0, 0.0).astype(BF16)
    end = slice(length - LANES, length)
    rim = remote(rim_out, rim_in, rim_send.at[0], rim_recv.at[0], ep=(me + 1) % ep_size)

    def send_rims():
        for name in ("x", "b", "c"):
            loads[name].wait()

        @pl.when(me + 1 < ep_size)
        def _():
            rim_out[:, :value_rows] = dot(edge, x_ref[:, end], ((1,), (1,))).astype(BF16)
            rim_out[:, value_rows : value_rows + NSTATE] = dot(edge, b_ref[group, end], ((1,), (1,))).astype(BF16)
            rim_out[:, value_rows + NSTATE :] = dot(edge, c_ref[group, end], ((1,), (1,))).astype(BF16)
            rim.start()

    def columns():
        for name in ("tapx", "tapb", "tapc", "dt", "rate", "hgain"):
            loads[name].wait()
        tap_col[...] = upright(tapx_ref[...])
        tapb_col[...] = upright(tapb_ref[...])
        tapc_col[...] = upright(tapc_ref[...])
        top = lax.broadcasted_iota(jnp.int32, (8, LANES), 0) == 0
        flat = jnp.broadcast_to(hgain_ref[...], (8, hgain_ref.shape[1]))
        gain_col[...] = dot(flat, jnp.where(top, 1.0, 0.0), ((0,), (0,)), lax.Precision.HIGHEST)

    def decays():
        step, cum, cum_col = prefix_decays(dt_ref, rate_ref)
        step_ref[...] = step
        cum_ref[...] = cum
        for head in range(heads):
            col_ref[head] = jnp.broadcast_to(cum_col[:, head : head + 1], (length, LANES))

    def open_rims():
        @pl.when(me > 0)
        def _():
            rim.wait_recv()
            xrim[...] = dot(rim_in[:, :value_rows], edge, ((0,), (0,)))
            brim[...] = dot(rim_in[:, value_rows : value_rows + NSTATE], edge, ((0,), (0,)))
            crim[...] = dot(rim_in[:, value_rows + NSTATE :], edge, ((0,), (0,)))

        @pl.when(me == 0)
        def _():
            for ref in (xrim, brim, crim):
                ref[...] = jnp.zeros_like(ref)

    def b_stream():
        bconv_ref[...] = conv_rows(b_ref[group, :], brim[...], tapb_col[group, :]).astype(BF16)

    def c_stream():
        cconv_ref[...] = conv_rows(c_ref[group, :], crim[...], tapc_col[group, :]).astype(BF16)

    def scores():
        score_ref[...] = dot(bconv_ref[...], cconv_ref[...], ((0,), (0,)))

    def turn(quarter):
        if quarter == 0:
            for name in ("gate", "up", "gate2", "up2", "down", "z"):
                loads[name].wait()
        cut = features // 4
        at = slice(quarter * cut, (quarter + 1) * cut)
        gut_ref[at, :] = gu_ref[:, at].T

    def split(reach):
        high = reach.astype(BF16).astype(F32)
        at = lax.broadcasted_iota(jnp.int32, (RIM, NSTATE), 0)
        wideness = (RIM, NSTATE)
        low = jnp.broadcast_to(reach - high, wideness)
        return jnp.where(at == 0, jnp.broadcast_to(high, wideness), jnp.where(at == 1, low, 0.0)).astype(BF16)

    def joinup(block):
        block = block.astype(F32)
        return block[0:1] + block[1:2]

    def end_state(head):
        rows = slice(head * HEAD_DIM, (head + 1) * HEAD_DIM)
        value = conv_rows(x_ref[rows, :], xrim[rows, :], tap_col[rows, :])
        own = cum_ref[head : head + 1, :]
        last = own[:, length - 1 :]
        xs = value * step_ref[head : head + 1, :]
        tail = xs * jnp.exp(last - own)
        pre1_out[head, :HEAD_DIM] = dot(tail.astype(BF16), bconv_ref[...], ((1,), (1,))).astype(BF16)
        pre1_out[head, HEAD_DIM:] = split(jnp.broadcast_to(jnp.exp(last), (1, NSTATE)))
        xs_ref[rows, :] = xs.astype(BF16)

    def local_y(head):
        rows = slice(head * HEAD_DIM, (head + 1) * HEAD_DIM)
        own = cum_ref[head : head + 1, :]
        brow = lax.broadcasted_iota(jnp.int32, (BLOCK, BLOCK), 0)
        bcol = lax.broadcasted_iota(jnp.int32, (BLOCK, BLOCK), 1)
        causal = brow <= bcol
        for target in range(length // BLOCK):
            at = slice(target * BLOCK, (target + 1) * BLOCK)
            pieces = []
            for source in range(target + 1):
                of = slice(source * BLOCK, (source + 1) * BLOCK)
                gap = own[:, at] - col_ref[head, of, :]
                if source == target:
                    gap = jnp.where(causal, gap, -jnp.inf)
                pieces.append((score_ref[of, at] * jnp.exp(gap)).astype(BF16))
            mask = pieces[0] if target == 0 else jnp.concatenate(pieces, axis=0)
            y_ref[rows, at] = dot(xs_ref[rows, : (target + 1) * BLOCK], mask, ((1,), (0,)))

    def close(head):
        if head == 0:
            for dx in range(1, ROWX):
                pre3(dx).wait_recv()
        rows = slice(head * HEAD_DIM, (head + 1) * HEAD_DIM)
        carried = dot(pre3_in[head], cconv_ref[...], ((1,), (0,)))
        y = y_ref[rows, :] + carried * jnp.exp(cum_ref[head : head + 1, :])
        gated = y * silu(z_ref[rows, :].astype(F32))
        norm = lax.rsqrt(jnp.mean(gated * gated, axis=0, keepdims=True) + HEAD_EPS)
        mixed_ref[rows, :] = (gated * norm * gain_col[rows, 0:1]).astype(BF16)

    def pre1(dx):
        head = (x + dx) % ROWX
        return remote(pre1_out.at[head], pre1_in.at[x], p1_send.at[dx], p1_recv.at[dx], ep=z * ROWX + head)

    def pre2(dz):
        return remote(pre2_out, pre2_in.at[z], p2_send.at[dz], p2_recv.at[dz], ep=((z + dz) % deep) * ROWX + x)

    def pre3(dx):
        spot = (x + dx) % ROWX
        return remote(pre3_out.at[spot], pre3_in.at[x], p3_send.at[dx], p3_recv.at[dx], ep=z * ROWX + spot)

    def spread_states():
        for dx in range(1, ROWX):
            pre1(dx).start()
        pre1_in[x] = pre1_out[x]

    def row_totals():
        for dx in range(1, ROWX):
            pre1(dx).wait_recv()
        total = jnp.zeros((HEAD_DIM, NSTATE), F32)
        reach = jnp.ones((1, NSTATE), F32)
        for spot in range(ROWX):
            ex_ref[spot] = total
            exr_ref[spot] = jnp.broadcast_to(reach, exr_ref.shape[1:])
            hold = joinup(pre1_in[spot, HEAD_DIM:])
            total = pre1_in[spot, :HEAD_DIM].astype(F32) + hold * total
            reach = reach * hold
        pre2_out[:HEAD_DIM] = total.astype(BF16)
        pre2_out[HEAD_DIM:] = split(reach)
        for dz in range(1, deep):

            @pl.when(z + dz < deep)
            def _(dz=dz):
                pre2(dz).start()

    def incoming():
        for dz in range(1, deep):

            @pl.when(z >= dz)
            def _(dz=dz):
                pre2(dz).wait_recv()

        prior = jnp.zeros((HEAD_DIM, NSTATE), F32)
        for level in range(deep - 1):
            after = pre2_in[level, :HEAD_DIM].astype(F32) + joinup(pre2_in[level, HEAD_DIM:]) * prior
            prior = jnp.where(level < z, after, prior)
        for spot in range(ROWX):
            pre3_out[spot] = (ex_ref[spot] + exr_ref[spot, 0:1] * prior).astype(BF16)
        for dx in range(1, ROWX):
            pre3(dx).start()
        pre3_in[x] = pre3_out[x]

    def at_rows(team, d, step):
        if step < far - 1:
            return team * span, span
        return team * span + d * half, half

    def ag(d, team, step):
        sign = 1 - 2 * d
        origin = ((chip + chips - sign * step) % chips) * 2 + core
        start, count = at_rows(team, d, step)
        ref = xall.at[origin, pl.ds(start, count), :]
        return remote(ref, ref, ag_send.at[d, team, step], ag_recv.at[d, team, step], tp=around[d])

    def sib(team, d, step):
        sign = 1 - 2 * d
        origin = ((chip + chips - sign * (step + 1)) % chips) * 2 + core
        start, count = at_rows(team, d, step)
        ref = xall.at[origin, pl.ds(start, count), :]
        index = 0 if step < 0 else 1 + d * far + step
        return remote(ref, ref, sib_send.at[team, index], sib_recv.at[team, index], tp=sibling)

    def arrivals():
        return [(0, -1)] + [(d, step) for step in range(far) for d in range(2)]

    def gather_own(team):
        for slot in range(GROUPED):
            if team or slot:
                box(team * GROUPED + slot).wait_recv()
        xall[lane, team * span : (team + 1) * span, :] = packed(landed, team)
        for d in range(2):
            ag(d, team, 0).start()
        sib(team, 0, -1).start()

    def gather_step(team, step):
        for d in range(2):
            ag(d, team, step).wait_recv()
            if step + 1 < far:
                ag(d, team, step + 1).start()
            sib(team, d, step).start()

    def ffn(team):
        for d, step in arrivals():
            sib(team, d, step).wait_recv()
        rows = slice(team * span, (team + 1) * span)
        tokens_in = jnp.concatenate([xall[i, rows, :] for i in range(tp_size)], axis=1)
        both = dot(tokens_in, gut_ref[...], ((1,), (0,)))
        hidden = (silu(both[:, :main]) * both[:, main : 2 * main]).astype(BF16)
        last = both[:, 2 * main :]
        extra = (silu(last) * pltpu.roll(last, rest, 1)).astype(BF16)[:, :rest]
        out = dot(jnp.concatenate([hidden, extra], axis=1), down_ref[...], ((1,), (0,)))
        for i in range(tp_size):
            part[team, i % 2, i // 2] = out[:, i * width : (i + 1) * width].astype(BF16)
        for reach in order_of_need:
            cross(team, reach).start()

    order_of_need = [far]
    for away in range(far - 1, 0, -1):
        order_of_need += [away, chips - away]
    order_of_need.append(0)

    def cross(team, reach):
        at = (chip + reach) % chips
        return remote(
            part.at[team, 1 - core, at], sibp.at[team, at], dd_send.at[team, reach], dd_recv.at[team, reach], tp=sibling
        )

    def own_sum(team, reach):
        at = (chip + reach) % chips
        return part[team, core, at].astype(F32) + sibp[team, at].astype(F32)

    def rs(d, team, step):
        start, count = (d * half, half) if step == 0 else (0, span)
        return remote(
            rs_out.at[d, team, step, pl.ds(start, count), :], rs_in.at[d, team, step, pl.ds(start, count), :],
            rs_send.at[d, team, step], rs_recv.at[d, team, step], tp=around[d],
        )

    def scatter_first(team):
        cross(team, far).wait_recv()
        total = own_sum(team, far).astype(BF16)
        for d in range(2):
            cut = slice(d * half, (d + 1) * half)
            rs_out[d, team, 0, cut, :] = total[cut]
            rs(d, team, 0).start()

    def scatter_step(team, step):
        for d in range(2):
            reach = far - step if d == 0 else chips - (far - step)
            cross(team, reach).wait_recv()
            total = own_sum(team, reach)
            rs(d, team, step - 1).wait_recv()
            if step == 1:
                cut = slice(d * half, (d + 1) * half)
                other = slice((1 - d) * half, (2 - d) * half)
                rs_out[d, team, step, other, :] = total[other].astype(BF16)
                rs_out[d, team, step, cut, :] = (total[cut] + rs_in[d, team, 0, cut, :].astype(F32)).astype(BF16)
            else:
                rs_out[d, team, step] = (total + rs_in[d, team, step - 1].astype(F32)).astype(BF16)
            rs(d, team, step).start()

    def scatter_last(team):
        cross(team, 0).wait_recv()
        total = own_sum(team, 0)
        for d in range(2):
            rs(d, team, far - 1).wait_recv()
            total = total + rs_in[d, team, far - 1].astype(F32)
        for slot in range(GROUPED):
            j = team * GROUPED + slot
            piece = total[slot * pad : (slot + 1) * pad].astype(BF16)
            if j:
                ret_out[j] = piece
                back(j).start()
            else:
                returned[j] = piece

    pl.semaphore_wait(barrier, ep_size - 1 + len(around) + 1)
    for team in (0, 2, 1, 3):
        dispatch(team)
    send_rims()
    parts = (
        columns, decays, turn, gather_own, gather_step, ffn, scatter_first, scatter_step, scatter_last, open_rims,
        b_stream, c_stream, scores, end_state, spread_states, local_y, row_totals, incoming, close,
    )
    named = {part.__name__: part for part in parts}
    for step in PLAN:
        named[step[0]](*step[1:])
    def combine():
        total = jnp.zeros((tokens, width), F32)
        for team in range(teams):
            for slot in range(GROUPED):
                if team or slot:
                    back(team * GROUPED + slot).wait_recv()
            total = total + dot(pick_ref[team * wide : (team + 1) * wide, :], packed(returned, team), ((0,), (0,)))
        moe_ref[...] = total.astype(BF16)

    combine()

    for j in range(1, ep_size):
        box(j).wait_send()
        back(j).wait_send()

    @pl.when(me + 1 < ep_size)
    def _():
        rim.wait_send()

    for dx in range(1, ROWX):
        pre1(dx).wait_send()
        pre3(dx).wait_send()
    for dz in range(1, deep):

        @pl.when(z + dz < deep)
        def _(dz=dz):
            pre2(dz).wait_send()

    for team in range(teams):
        for d in range(2):
            for step in range(far):
                ag(d, team, step).wait_send()
                rs(d, team, step).wait_send()
        for d, step in arrivals():
            sib(team, d, step).wait_send()
        for reach in range(chips):
            cross(team, reach).wait_send()


def emit_kernel(mixed_ref, moe_ref, mixed_out, moe_out, sems):
    copies = [
        pltpu.make_async_copy(mixed_ref, mixed_out, sems.at[0]),
        pltpu.make_async_copy(moe_ref, moe_out, sems.at[1]),
    ]
    for copy in copies:
        copy.start()
    for copy in copies:
        copy.wait()


def on_device(
    x_in, z_in, dt_raw, decay_rate, b_in, c_in, conv_x, conv_b, conv_c, head_gain,
    moe_rows, moe_gain, routes, route_logit, w_gate, w_up, w_down,
):
    heads, length = dt_raw.shape
    value_rows = x_in.shape[0]
    taps = conv_x.shape[1]
    tp_size = lax.axis_size("tp")
    ep_size = lax.axis_size("ep")
    tokens, features = moe_rows.shape
    top = routes.shape[1]
    capacity = 2 * tokens * top // ep_size
    pad = capacity
    width = features // tp_size
    hidden_units = w_gate.shape[2]
    slots = ep_size * capacity
    deep, chips = ep_size // ROWX, tp_size // 2
    far, teams, span = chips // 2, ep_size // GROUPED, GROUPED * capacity
    dma = pltpu.SemaphoreType.DMA
    shape = jax.ShapeDtypeStruct
    groups = b_in.shape[0]

    mixed, moe = pl.pallas_call(
        functools.partial(layer_kernel, ep_size=ep_size, tp_size=tp_size),
        out_shape=(VMEM((value_rows, length), BF16), VMEM((tokens, width), BF16)),
        in_specs=[pl.BlockSpec(memory_space=pltpu.HBM)] * 17,
        out_specs=tuple(vmem_specs(2)),
        scratch_shapes=[
            VMEM((tokens, features), BF16), VMEM((1, features), F32), VMEM((top, tokens), jnp.int32), VMEM((top, tokens), F32),
            VMEM((value_rows, length), BF16), VMEM((taps, value_rows), F32),
            VMEM((groups, length), BF16), VMEM((taps, groups), F32), VMEM((groups, length), BF16), VMEM((taps, groups), F32),
            VMEM((heads, length), F32), VMEM((1, heads), F32), VMEM((value_rows, length), BF16), VMEM((1, value_rows), F32),
            VMEM((2 * hidden_units, features), BF16), VMEM((features, 2 * hidden_units), BF16), VMEM((hidden_units, features), BF16),
            VMEM((ep_size, tokens), F32), VMEM((ep_size, tokens), F32), VMEM((ep_size * pad, tokens), BF16),
            VMEM((ep_size, pad, width), BF16), VMEM((ep_size, pad, width), BF16),
            VMEM((tp_size, slots, width), BF16),
            VMEM((teams, 2, chips, span, width), BF16), VMEM((teams, chips, span, width), BF16),
            VMEM((2, teams, far, span, width), BF16), VMEM((2, teams, far, span, width), BF16),
            VMEM((ep_size, pad, width), BF16), VMEM((ep_size, pad, width), BF16),
            VMEM((RIM, value_rows + 2 * NSTATE), BF16), VMEM((RIM, value_rows + 2 * NSTATE), BF16),
            VMEM((value_rows, LANES), F32), VMEM((NSTATE, LANES), F32), VMEM((NSTATE, LANES), F32),
            VMEM((value_rows, taps), F32), VMEM((groups, taps), F32), VMEM((groups, taps), F32),
            VMEM((value_rows, LANES), F32),
            VMEM((heads, length), F32), VMEM((heads, length), F32), VMEM((heads, length, LANES), F32),
            VMEM((length, length), F32), VMEM((NSTATE, length), BF16), VMEM((NSTATE, length), BF16),
            VMEM((value_rows, length), BF16), VMEM((value_rows, length), F32),
            VMEM((heads, PACK, NSTATE), BF16), VMEM((ROWX, PACK, NSTATE), BF16),
            VMEM((PACK, NSTATE), BF16), VMEM((deep, PACK, NSTATE), BF16),
            VMEM((ROWX, HEAD_DIM, NSTATE), BF16), VMEM((ROWX, HEAD_DIM, NSTATE), BF16),
            VMEM((ROWX, HEAD_DIM, NSTATE), F32), VMEM((ROWX, 8, NSTATE), F32),
            dma((19,)), dma((ep_size,)), dma((ep_size,)), dma((1,)), dma((1,)),
            dma((2, teams, far)), dma((2, teams, far)), dma((teams, 1 + 2 * far)), dma((teams, 1 + 2 * far)),
            dma((teams, chips)), dma((teams, chips)), dma((2, teams, far)), dma((2, teams, far)),
            dma((ep_size,)), dma((ep_size,)), dma((ROWX,)), dma((ROWX,)), dma((deep,)), dma((deep,)), dma((ROWX,)), dma((ROWX,)),
        ],
        compiler_params=pltpu.CompilerParams(collective_id=0, has_side_effects=True, vmem_limit_bytes=60 * 2**20),
        name="layer",
    )(
        moe_rows, moe_gain.reshape(1, features), routes.T, route_logit.T,
        x_in, conv_x.T, b_in, conv_b.T, c_in, conv_c.T, dt_raw, decay_rate.reshape(1, heads),
        z_in, head_gain.reshape(1, value_rows),
        jnp.swapaxes(w_gate, 1, 2), jnp.swapaxes(w_up, 1, 2), w_down,
    )
    mixed, moe = pl.pallas_call(
        emit_kernel,
        out_shape=(shape((value_rows, length), BF16), shape((tokens, width), BF16)),
        in_specs=vmem_specs(2),
        out_specs=tuple([pl.BlockSpec(memory_space=pltpu.HBM)] * 2),
        scratch_shapes=[dma((2,))],
        compiler_params=pltpu.CompilerParams(vmem_limit_bytes=8 * 2**20),
        name="emit",
    )(mixed, moe)
    return (mixed, moe.T)


def solution(mesh):
    return jax.shard_map(
        on_device,
        mesh=mesh,
        in_specs=(
            P("tp", "ep"), P("tp", "ep"), P("tp", "ep"), P("tp"), P(None, "ep"), P(None, "ep"),
            P("tp", None), P(), P(), P("tp"), P("ep", None), P(), P("ep", None), P("ep", None),
            P("ep", None, "tp"), P("ep", None, "tp"), P("ep", "tp", None),
        ),
        out_specs=(P("tp", "ep"), P("tp", "ep")),
        check_vma=False,
    )
```

```python
import functools
import jax
import jax.numpy as jnp
from jax import lax
from jax.experimental import pallas as pl
from jax.experimental.pallas import tpu as pltpu
from jax.sharding import PartitionSpec as P

HEADS = 64
HEAD_DIM = 64
GROUPS = 2
NSTATE = 128
BLOCK = 128
ROW_EPS = 0.1
HEAD_EPS = 1.0
LANES = 128
F32 = jnp.float32
BF16 = jnp.bfloat16
ROWX = 4
GROUPED = 8
RIM = 16
PACK = 80
PLAN = (
    ("columns",), ("decays",), ("turn", 0), ("turn", 1), ("turn", 2), ("turn", 3), ("gather_own", 0), ("open_rims",),
    ("gather_own", 1), ("b_stream",), ("c_stream",), ("end_state", 0), ("end_state", 1), ("gather_step", 0, 0),
    ("end_state", 2), ("end_state", 3), ("scores",), ("gather_own", 2), ("spread_states",), ("local_y", 0),
    ("local_y", 1), ("gather_own", 3), ("local_y", 2), ("gather_step", 1, 0), ("local_y", 3), ("gather_step", 0, 1),
    ("gather_step", 2, 0), ("gather_step", 3, 0), ("gather_step", 1, 1), ("gather_step", 0, 3), ("gather_step", 0, 2),
    ("row_totals",), ("gather_step", 2, 1), ("ffn", 0), ("gather_step", 3, 1), ("gather_step", 1, 3),
    ("gather_step", 1, 2), ("scatter_first", 0), ("ffn", 1), ("gather_step", 2, 3), ("gather_step", 2, 2),
    ("gather_step", 3, 3), ("gather_step", 3, 2), ("incoming",), ("scatter_first", 1), ("ffn", 2),
    ("scatter_step", 0, 2), ("ffn", 3), ("scatter_first", 2), ("scatter_first", 3), ("scatter_step", 1, 2),
    ("scatter_step", 0, 3), ("close", 0), ("close", 1), ("close", 2), ("close", 3), ("scatter_step", 2, 2),
    ("scatter_step", 3, 2), ("scatter_step", 1, 3), ("scatter_last", 0), ("scatter_step", 2, 3),
    ("scatter_step", 3, 3), ("scatter_last", 1), ("scatter_last", 2), ("scatter_last", 3),
)
VMEM = pltpu.VMEM
MESH = pl.DeviceIdType.MESH


def vmem_specs(count):
    return [pl.BlockSpec(memory_space=VMEM)] * count


def cost(flops, moved):
    return pl.CostEstimate(flops=flops, bytes_accessed=moved, transcendentals=0)


def dot(a, b, dims, precision=None):
    return lax.dot_general(a, b, (dims, ((), ())), preferred_element_type=F32, precision=precision)


def eye(count):
    row = lax.broadcasted_iota(jnp.int32, (count, count), 0)
    col = lax.broadcasted_iota(jnp.int32, (count, count), 1)
    return jnp.where(row == col, 1.0, 0.0).astype(F32)


def upright(flat):
    return dot(flat, eye(flat.shape[0]), ((0,), (0,)), lax.Precision.HIGHEST)


def silu(v):
    return v / (1.0 + jnp.exp(-v))


def conv_rows(signal, rim, weight):
    taps = weight.shape[1]
    joined = jnp.concatenate([rim.astype(F32), signal.astype(F32)], axis=1)
    running = weight[:, taps - 1 : taps] * joined[:, LANES:]
    for back in range(1, taps):
        moved = pltpu.roll(joined, back, 1)[:, LANES:]
        running = running + weight[:, taps - 1 - back : taps - back] * moved
    return silu(running)


def prefix_decays(dt_ref, rate_ref):
    dt = dt_ref[...]
    step = jnp.maximum(dt, 0.0) + jnp.log1p(jnp.exp(-jnp.abs(dt)))
    rate = jnp.where(eye(dt.shape[0]) > 0.0, rate_ref[...], 0.0)
    log_decay = -step * jnp.sum(rate, axis=1, keepdims=True)
    length = dt.shape[1]
    row = lax.broadcasted_iota(jnp.int32, (length, length), 0)
    col = lax.broadcasted_iota(jnp.int32, (length, length), 1)
    upper = jnp.where(row <= col, 1.0, 0.0).astype(F32)
    lower = jnp.where(row >= col, 1.0, 0.0).astype(F32)
    high = lax.Precision.HIGHEST
    cum = dot(log_decay, upper, ((1,), (0,)), high)
    cum_col = dot(lower, log_decay, ((1,), (1,)), high)
    return step, cum, cum_col


def remote(source, target, send, recv, **where):
    return pltpu.make_async_remote_copy(
        src_ref=source, dst_ref=target, send_sem=send, recv_sem=recv, device_id=where, device_id_type=MESH
    )


def offsets(ep_size):
    deep = ep_size // ROWX
    hops = [(dz, dx) for dz in range(deep) for dx in range(ROWX)]
    near = sorted(hops, key=lambda h: min(h[0], deep - h[0]) + min(h[1], ROWX - h[1]))
    first, second = near[:GROUPED], near[GROUPED : 2 * GROUPED]
    return first + second + near[3 * GROUPED :] + near[2 * GROUPED : 3 * GROUPED]


def layer_kernel(
    rows_hbm, gain_hbm, routes_hbm, logit_hbm, x_hbm, tapx_hbm, b_hbm, tapb_hbm, c_hbm, tapc_hbm,
    dt_hbm, rate_hbm, z_hbm, hgain_hbm, gate_hbm, up_hbm, down_hbm,
    mixed_ref, moe_ref,
    rows_ref, gain_ref, routes_ref, logit_ref, x_ref, tapx_ref, b_ref, tapb_ref, c_ref, tapc_ref,
    dt_ref, rate_ref, z_ref, hgain_ref, gu_ref, gut_ref, down_ref,
    rank_ref, weight_ref, pick_ref, outbox, landed, xall, part, sibp, rs_out, rs_in,
    ret_out, returned,
    rim_out, rim_in, xrim, brim, crim, tap_col, tapb_col, tapc_col, gain_col,
    step_ref, cum_ref, col_ref, score_ref, bconv_ref, cconv_ref, xs_ref, y_ref,
    pre1_out, pre1_in, pre2_out, pre2_in, pre3_out, pre3_in, ex_ref, exr_ref, sum_ref,
    in_sem, box_send, box_recv, rim_send, rim_recv, ag_send, ag_recv, sib_send, sib_recv,
    dd_send, dd_recv, rs_send, rs_recv, ret_send, ret_recv, p1_send, p1_recv, p2_send, p2_recv, p3_send, p3_recv,
    *, ep_size, tp_size,
):
    me, lane = lax.axis_index("ep"), lax.axis_index("tp")
    deep, chips = ep_size // ROWX, tp_size // 2
    far = chips // 2
    z, x = me // ROWX, me % ROWX
    chip, core = lane // 2, lane % 2
    tokens, features = rows_ref.shape
    width = features // tp_size
    heads, length = dt_ref.shape
    pad = outbox.shape[1]
    capacity = xall.shape[1] // ep_size
    hops = offsets(ep_size)
    teams = ep_size // GROUPED
    span = GROUPED * capacity
    half = span // 2
    wide = GROUPED * pad

    barrier = pltpu.get_barrier_semaphore()
    for hop in range(1, ep_size):
        pl.semaphore_signal(barrier, 1, device_id={"ep": (me + hop) % ep_size}, device_id_type=MESH)
    around = [((chip + 1) % chips) * 2 + core, ((chip + chips - 1) % chips) * 2 + core]
    beyond = [((chip + 2) % chips) * 2 + core, ((chip + chips - 2) % chips) * 2 + core]
    sibling = chip * 2 + 1 - core
    for other in around + beyond + [sibling]:
        pl.semaphore_signal(barrier, 1, device_id={"tp": other}, device_id_type=MESH)

    loads = {}

    def load(name, source, target):
        copy = pltpu.make_async_copy(source, target, in_sem.at[len(loads)])
        copy.start()
        loads[name] = copy

    load("rows", rows_hbm, rows_ref)
    load("routes", routes_hbm, routes_ref)
    load("logit", logit_hbm, logit_ref)
    load("gain", gain_hbm, gain_ref)
    load("x", x_hbm, x_ref)
    load("b", b_hbm, b_ref)
    load("c", c_hbm, c_ref)
    load("tapx", tapx_hbm, tapx_ref)
    load("tapb", tapb_hbm, tapb_ref)
    load("tapc", tapc_hbm, tapc_ref)
    load("dt", dt_hbm, dt_ref)
    load("rate", rate_hbm, rate_ref)
    hidden_units = down_ref.shape[0]
    main = hidden_units // 256 * 256
    rest = hidden_units - main
    load("gate", gate_hbm.at[0, pl.ds(0, main), :], gu_ref.at[pl.ds(0, main), :])
    load("up", up_hbm.at[0, pl.ds(0, main), :], gu_ref.at[pl.ds(main, main), :])
    load("gate2", gate_hbm.at[0, pl.ds(main, rest), :], gu_ref.at[pl.ds(2 * main, rest), :])
    load("up2", up_hbm.at[0, pl.ds(main, rest), :], gu_ref.at[pl.ds(2 * main + rest, rest), :])
    load("down", down_hbm.at[0], down_ref)
    load("z", z_hbm, z_ref)
    load("hgain", hgain_hbm, hgain_ref)

    for name in ("routes", "logit"):
        loads[name].wait()
    routes = routes_ref[...]
    logit = logit_ref[...]
    first = 1.0 / (1.0 + jnp.exp(logit[1:2] - logit[0:1]))
    second = 1.0 / (1.0 + jnp.exp(logit[0:1] - logit[1:2]))
    number = lax.broadcasted_iota(jnp.int32, (ep_size, tokens), 0)
    in_first = number == routes[0:1]
    in_second = number == routes[1:2]
    hits = jnp.where(in_first, 1.0, 0.0) + jnp.where(in_second, 1.0, 0.0)
    row = lax.broadcasted_iota(jnp.int32, (tokens, tokens), 0)
    col = lax.broadcasted_iota(jnp.int32, (tokens, tokens), 1)
    earlier = jnp.where(row < col, 1.0, 0.0).astype(BF16)
    rank = dot(hits.astype(BF16), earlier, ((1,), (0,)))
    weight_ref[...] = jnp.where(in_first, first, 0.0) + jnp.where(in_second, second, 0.0)
    rank_ref[...] = jnp.where(hits > 0.0, rank, -1.0)
    for name in ("rows", "gain"):
        loads[name].wait()
    values = rows_ref[...].astype(F32)
    scale = lax.rsqrt(jnp.mean(values * values, axis=1, keepdims=True) + ROW_EPS)
    mine = pl.ds(pl.multiple_of(lane * width, LANES), width)
    normed = (rows_ref[:, mine].astype(F32) * scale * gain_ref[:, mine]).astype(BF16)
    place = lax.broadcasted_iota(jnp.int32, (pad, tokens), 0).astype(F32)

    def arrived(ref, sem):
        remote(ref, ref, in_sem.at[0], sem, tp=sibling).wait_recv()

    def gone(ref, sem):
        remote(ref, ref, sem, in_sem.at[0], tp=sibling).wait_send()

    def ahead(j):
        dz, dx = hops[j]
        return ((z + dz) % deep) * ROWX + (x + dx) % ROWX

    def behind(j):
        dz, dx = hops[j]
        return ((z + deep - dz) % deep) * ROWX + (x + ROWX - dx) % ROWX

    def box(j):
        return remote(outbox.at[j], landed.at[j], box_send.at[0], box_recv.at[j // GROUPED], ep=ahead(j))

    def back(j):
        return remote(ret_out.at[j], returned.at[j], ret_send.at[0], ret_recv.at[j // GROUPED], ep=behind(j))

    def dispatch(team):
        ones = []
        picks = []
        for slot in range(GROUPED):
            expert = ahead(team * GROUPED + slot)
            same = place == rank_ref[pl.ds(expert, 1), :]
            ones.append(jnp.where(same, 1.0, 0.0))
            picks.append(jnp.where(same, weight_ref[pl.ds(expert, 1), :], 0.0))
        pick_ref[team * wide : (team + 1) * wide, :] = jnp.concatenate(picks, axis=0).astype(BF16)
        chosen = dot(jnp.concatenate(ones, axis=0).astype(BF16), normed, ((1,), (0,)))
        for slot in range(GROUPED):
            j = team * GROUPED + slot
            piece = chosen[slot * pad : (slot + 1) * pad].astype(BF16)
            if j:
                outbox[j] = piece
                box(j).start()
            else:
                landed[j] = piece

    def received(ref, team):
        skip = 1 if team == 0 else 0
        return ref.at[pl.ds(team * GROUPED + skip, GROUPED - skip)]

    def packed(ref, team):
        pieces = [ref[team * GROUPED + slot].astype(F32) for slot in range(GROUPED)]
        return jnp.concatenate(pieces, axis=0).astype(BF16)

    group = pl.ds(pl.multiple_of(lane * heads // (HEADS // GROUPS) * NSTATE, NSTATE), NSTATE)
    value_rows = x_ref.shape[0]
    pickrow = lax.broadcasted_iota(jnp.int32, (RIM, LANES), 0)
    picklane = lax.broadcasted_iota(jnp.int32, (RIM, LANES), 1)
    edge = jnp.where(picklane == pickrow + (LANES - RIM), 1.0, 0.0).astype(BF16)
    end = slice(length - LANES, length)
    rim = remote(rim_out, rim_in, rim_send.at[0], rim_recv.at[0], ep=(me + 1) % ep_size)

    def send_rims():
        for name in ("x", "b", "c"):
            loads[name].wait()

        @pl.when(me + 1 < ep_size)
        def _():
            rim_out[:, :value_rows] = dot(edge, x_ref[:, end], ((1,), (1,))).astype(BF16)
            rim_out[:, value_rows : value_rows + NSTATE] = dot(edge, b_ref[group, end], ((1,), (1,))).astype(BF16)
            rim_out[:, value_rows + NSTATE :] = dot(edge, c_ref[group, end], ((1,), (1,))).astype(BF16)
            rim.start()

    def columns():
        for name in ("tapx", "tapb", "tapc", "dt", "rate", "hgain"):
            loads[name].wait()
        tap_col[...] = upright(tapx_ref[...])
        tapb_col[...] = upright(tapb_ref[...])
        tapc_col[...] = upright(tapc_ref[...])
        top = lax.broadcasted_iota(jnp.int32, (8, LANES), 0) == 0
        flat = jnp.broadcast_to(hgain_ref[...], (8, hgain_ref.shape[1]))
        gain_col[...] = dot(flat, jnp.where(top, 1.0, 0.0), ((0,), (0,)), lax.Precision.HIGHEST)

    def decays():
        step, cum, cum_col = prefix_decays(dt_ref, rate_ref)
        step_ref[...] = step
        cum_ref[...] = cum
        for head in range(heads):
            col_ref[head] = jnp.broadcast_to(cum_col[:, head : head + 1], (length, LANES))

    def open_rims():
        @pl.when(me > 0)
        def _():
            rim.wait_recv()
            xrim[...] = dot(rim_in[:, :value_rows], edge, ((0,), (0,)))
            brim[...] = dot(rim_in[:, value_rows : value_rows + NSTATE], edge, ((0,), (0,)))
            crim[...] = dot(rim_in[:, value_rows + NSTATE :], edge, ((0,), (0,)))

        @pl.when(me == 0)
        def _():
            for ref in (xrim, brim, crim):
                ref[...] = jnp.zeros_like(ref)

    def b_stream():
        bconv_ref[...] = conv_rows(b_ref[group, :], brim[...], tapb_col[group, :]).astype(BF16)

    def c_stream():
        cconv_ref[...] = conv_rows(c_ref[group, :], crim[...], tapc_col[group, :]).astype(BF16)

    def scores():
        score_ref[...] = dot(bconv_ref[...], cconv_ref[...], ((0,), (0,)))

    def turn(quarter):
        if quarter == 0:
            for name in ("gate", "up", "gate2", "up2", "down", "z"):
                loads[name].wait()
        cut = features // 4
        at = slice(quarter * cut, (quarter + 1) * cut)
        gut_ref[at, :] = gu_ref[:, at].T

    def split(reach):
        high = reach.astype(BF16).astype(F32)
        at = lax.broadcasted_iota(jnp.int32, (RIM, NSTATE), 0)
        wideness = (RIM, NSTATE)
        low = jnp.broadcast_to(reach - high, wideness)
        return jnp.where(at == 0, jnp.broadcast_to(high, wideness), jnp.where(at == 1, low, 0.0)).astype(BF16)

    def joinup(block):
        block = block.astype(F32)
        return block[0:1] + block[1:2]

    def end_state(head):
        rows = slice(head * HEAD_DIM, (head + 1) * HEAD_DIM)
        value = conv_rows(x_ref[rows, :], xrim[rows, :], tap_col[rows, :])
        own = cum_ref[head : head + 1, :]
        last = own[:, length - 1 :]
        xs = value * step_ref[head : head + 1, :]
        tail = xs * jnp.exp(last - own)
        pre1_out[head, :HEAD_DIM] = dot(tail.astype(BF16), bconv_ref[...], ((1,), (1,))).astype(BF16)
        pre1_out[head, HEAD_DIM:] = split(jnp.broadcast_to(jnp.exp(last), (1, NSTATE)))
        xs_ref[rows, :] = xs.astype(BF16)

    def local_y(head):
        rows = slice(head * HEAD_DIM, (head + 1) * HEAD_DIM)
        own = cum_ref[head : head + 1, :]
        brow = lax.broadcasted_iota(jnp.int32, (BLOCK, BLOCK), 0)
        bcol = lax.broadcasted_iota(jnp.int32, (BLOCK, BLOCK), 1)
        causal = brow <= bcol
        for target in range(length // BLOCK):
            at = slice(target * BLOCK, (target + 1) * BLOCK)
            pieces = []
            for source in range(target + 1):
                of = slice(source * BLOCK, (source + 1) * BLOCK)
                gap = own[:, at] - col_ref[head, of, :]
                if source == target:
                    gap = jnp.where(causal, gap, -jnp.inf)
                pieces.append((score_ref[of, at] * jnp.exp(gap)).astype(BF16))
            mask = pieces[0] if target == 0 else jnp.concatenate(pieces, axis=0)
            y_ref[rows, at] = dot(xs_ref[rows, : (target + 1) * BLOCK], mask, ((1,), (0,)))

    def close(head):
        if head == 0:
            arrived(pre3_in.at[pl.ds(0, ROWX - 1)], p3_recv.at[0])
        rows = slice(head * HEAD_DIM, (head + 1) * HEAD_DIM)
        carried = dot(pre3_in[head], cconv_ref[...], ((1,), (0,)))
        y = y_ref[rows, :] + carried * jnp.exp(cum_ref[head : head + 1, :])
        gated = y * silu(z_ref[rows, :].astype(F32))
        norm = lax.rsqrt(jnp.mean(gated * gated, axis=0, keepdims=True) + HEAD_EPS)
        mixed_ref[rows, :] = (gated * norm * gain_col[rows, 0:1]).astype(BF16)

    def pre1(dx):
        head = (x + dx) % ROWX
        return remote(pre1_out.at[head], pre1_in.at[x], p1_send.at[0], p1_recv.at[0], ep=z * ROWX + head)

    def pre2(dz):
        return remote(pre2_out, pre2_in.at[z], p2_send.at[dz], p2_recv.at[dz], ep=((z + dz) % deep) * ROWX + x)

    def pre3(dx):
        spot = (x + dx) % ROWX
        return remote(pre3_out.at[spot], pre3_in.at[x], p3_send.at[0], p3_recv.at[0], ep=z * ROWX + spot)

    def spread_states():
        for dx in range(1, ROWX):
            pre1(dx).start()
        pre1_in[x] = pre1_out[x]

    def row_totals():
        arrived(pre1_in.at[pl.ds(0, ROWX - 1)], p1_recv.at[0])
        total = jnp.zeros((HEAD_DIM, NSTATE), F32)
        reach = jnp.ones((1, NSTATE), F32)
        for spot in range(ROWX):
            ex_ref[spot] = total
            exr_ref[spot] = jnp.broadcast_to(reach, exr_ref.shape[1:])
            hold = joinup(pre1_in[spot, HEAD_DIM:])
            total = pre1_in[spot, :HEAD_DIM].astype(F32) + hold * total
            reach = reach * hold
        pre2_out[:HEAD_DIM] = total.astype(BF16)
        pre2_out[HEAD_DIM:] = split(reach)
        for dz in range(1, deep):

            @pl.when(z + dz < deep)
            def _(dz=dz):
                pre2(dz).start()

    def incoming():
        for dz in range(1, deep):

            @pl.when(z >= dz)
            def _(dz=dz):
                pre2(dz).wait_recv()

        prior = jnp.zeros((HEAD_DIM, NSTATE), F32)
        for level in range(deep - 1):
            after = pre2_in[level, :HEAD_DIM].astype(F32) + joinup(pre2_in[level, HEAD_DIM:]) * prior
            prior = jnp.where(level < z, after, prior)
        for spot in range(ROWX):
            pre3_out[spot] = (ex_ref[spot] + exr_ref[spot, 0:1] * prior).astype(BF16)
        for dx in range(1, ROWX):
            pre3(dx).start()
        pre3_in[x] = pre3_out[x]

    def at_rows(team, d, step):
        if step < far - 1:
            return team * span, span
        return team * span + d * half, half

    def ag(d, team, step):
        sign = 1 - 2 * d
        hop = min(step, far - 2)
        origin = ((chip + chips - sign * hop) % chips) * 2 + core
        start, count = at_rows(team, d, step)
        ref = xall.at[origin, pl.ds(start, count), :]
        target = around[d] if step < far - 1 else beyond[d]
        return remote(ref, ref, ag_send.at[0], ag_recv.at[team, step], tp=target)

    def sib(team, d, step):
        sign = 1 - 2 * d
        origin = ((chip + chips - sign * (step + 1)) % chips) * 2 + core
        start, count = at_rows(team, d, step)
        ref = xall.at[origin, pl.ds(start, count), :]
        return remote(ref, ref, sib_send.at[0], sib_recv.at[team], tp=sibling)

    def gather_own(team):
        arrived(received(landed, team), box_recv.at[team])
        xall[lane, team * span : (team + 1) * span, :] = packed(landed, team)
        for d in range(2):
            ag(d, team, 0).start()
        sib(team, 0, -1).start()

    def gather_step(team, step):
        arrived(xall.at[0, pl.ds(0, 2 * at_rows(team, 0, step)[1]), :], ag_recv.at[team, step])
        for d in range(2):
            if step + 1 < far - 1:
                ag(d, team, step + 1).start()
        for d in range(2):
            if step == far - 3:
                ag(d, team, far - 1).start()
            sib(team, d, step).start()

    def ffn(team):
        arrived(xall.at[pl.ds(0, chips // teams)], sib_recv.at[team])
        rows = slice(team * span, (team + 1) * span)
        tokens_in = jnp.concatenate([xall[i, rows, :] for i in range(tp_size)], axis=1)
        both = dot(tokens_in, gut_ref[...], ((1,), (0,)))
        hidden = (silu(both[:, :main]) * both[:, main : 2 * main]).astype(BF16)
        last = both[:, 2 * main :]
        extra = (silu(last) * pltpu.roll(last, rest, 1)).astype(BF16)[:, :rest]
        out = dot(jnp.concatenate([hidden, extra], axis=1), down_ref[...], ((1,), (0,)))
        for i in range(tp_size):
            part[team, i % 2, i // 2] = out[:, i * width : (i + 1) * width].astype(BF16)
        cross(team).start()

    def cross(team):
        return remote(part.at[team, 1 - core], sibp.at[team], dd_send.at[0], dd_recv.at[team], tp=sibling)

    def own_sum(team, reach):
        at = (chip + reach) % chips
        return part[team, core, at].astype(F32) + sibp[team, at].astype(F32)

    def rs(d, team, step):
        start, count = (d * half, half) if step == 0 else (0, span)
        return remote(
            rs_out.at[d, team, step, pl.ds(start, count), :], rs_in.at[d, team, step, pl.ds(start, count), :],
            rs_send.at[0], rs_recv.at[team, max(step - 1, 0)], tp=around[d] if step else beyond[d],
        )

    def reach_of(d, away):
        return away if d == 0 else chips - away

    def scatter_first(team):
        cross(team).wait_recv()
        for d in range(2):
            rs_out[d, team, 1] = own_sum(team, reach_of(d, far - 1)).astype(BF16)
            rs(d, team, 1).start()
        total = own_sum(team, far).astype(BF16)
        for d in range(2):
            cut = slice(d * half, (d + 1) * half)
            rs_out[d, team, 0, cut, :] = total[cut]
            rs(d, team, 0).start()

    def scatter_step(team, step):
        count = 3 * span if step == 2 else 2 * span
        arrived(xall.at[0, pl.ds(0, count), :], rs_recv.at[team, step - 2])
        for d in range(2):
            total = own_sum(team, reach_of(d, far - step)) + rs_in[d, team, step - 1].astype(F32)
            if step == 2:
                cut = slice(d * half, (d + 1) * half)
                other = slice((1 - d) * half, (2 - d) * half)
                rs_out[d, team, step, other, :] = total[other].astype(BF16)
                rs_out[d, team, step, cut, :] = (total[cut] + rs_in[d, team, 0, cut, :].astype(F32)).astype(BF16)
            else:
                rs_out[d, team, step] = total.astype(BF16)
            rs(d, team, step).start()

    def scatter_last(team):
        total = own_sum(team, 0)
        arrived(xall.at[0, pl.ds(0, 2 * span), :], rs_recv.at[team, far - 2])
        for d in range(2):
            total = total + rs_in[d, team, far - 1].astype(F32)
        for slot in range(GROUPED):
            j = team * GROUPED + slot
            piece = total[slot * pad : (slot + 1) * pad].astype(BF16)
            if j:
                ret_out[j] = piece
                back(j).start()
            else:
                returned[j] = piece

    pl.semaphore_wait(barrier, ep_size - 1 + len(around) + len(beyond) + 1)
    for team in range(teams):
        dispatch(team)
    send_rims()
    parts = (
        columns, decays, turn, gather_own, gather_step, ffn, scatter_first, scatter_step, scatter_last, open_rims,
        b_stream, c_stream, scores, end_state, spread_states, local_y, row_totals, incoming, close,
    )
    named = {part.__name__: part for part in parts}
    for step in PLAN:
        named[step[0]](*step[1:])
    def combine(team):
        arrived(received(returned, team), ret_recv.at[team])
        now = dot(pick_ref[team * wide : (team + 1) * wide, :], packed(returned, team), ((0,), (0,)))
        if team == 0:
            sum_ref[...] = now
        elif team + 1 < teams:
            sum_ref[...] = sum_ref[...] + now
        else:
            moe_ref[...] = (sum_ref[...] + now).astype(BF16)

    for team in range(teams):
        combine(team)

    gone(outbox.at[pl.ds(1, ep_size - 1)], box_send.at[0])
    gone(ret_out.at[pl.ds(1, ep_size - 1)], ret_send.at[0])
    gone(xall.at[pl.ds(0, chips - 1)], ag_send.at[0])
    gone(xall.at[pl.ds(0, chips - 1)], rs_send.at[0])
    gone(xall.at[pl.ds(0, chips)], sib_send.at[0])
    gone(xall.at[pl.ds(0, chips)], dd_send.at[0])
    gone(pre1_out.at[pl.ds(0, ROWX - 1)], p1_send.at[0])
    gone(pre3_out.at[pl.ds(0, ROWX - 1)], p3_send.at[0])

    @pl.when(me + 1 < ep_size)
    def _():
        rim.wait_send()

    for dz in range(1, deep):

        @pl.when(z + dz < deep)
        def _(dz=dz):
            pre2(dz).wait_send()


def emit_kernel(mixed_ref, moe_ref, mixed_out, moe_out, sems):
    copies = [
        pltpu.make_async_copy(mixed_ref, mixed_out, sems.at[0]),
        pltpu.make_async_copy(moe_ref, moe_out, sems.at[1]),
    ]
    for copy in copies:
        copy.start()
    for copy in copies:
        copy.wait()


def on_device(
    x_in, z_in, dt_raw, decay_rate, b_in, c_in, conv_x, conv_b, conv_c, head_gain,
    moe_rows, moe_gain, routes, route_logit, w_gate, w_up, w_down,
):
    heads, length = dt_raw.shape
    value_rows = x_in.shape[0]
    taps = conv_x.shape[1]
    tp_size = lax.axis_size("tp")
    ep_size = lax.axis_size("ep")
    tokens, features = moe_rows.shape
    top = routes.shape[1]
    capacity = 2 * tokens * top // ep_size
    pad = capacity
    width = features // tp_size
    hidden_units = w_gate.shape[2]
    slots = ep_size * capacity
    deep, chips = ep_size // ROWX, tp_size // 2
    far, teams, span = chips // 2, ep_size // GROUPED, GROUPED * capacity
    dma = pltpu.SemaphoreType.DMA
    shape = jax.ShapeDtypeStruct
    groups = b_in.shape[0]

    mixed, moe = pl.pallas_call(
        functools.partial(layer_kernel, ep_size=ep_size, tp_size=tp_size),
        out_shape=(VMEM((value_rows, length), BF16), VMEM((tokens, width), BF16)),
        in_specs=[pl.BlockSpec(memory_space=pltpu.HBM)] * 17,
        out_specs=tuple(vmem_specs(2)),
        scratch_shapes=[
            VMEM((tokens, features), BF16), VMEM((1, features), F32), VMEM((top, tokens), jnp.int32), VMEM((top, tokens), F32),
            VMEM((value_rows, length), BF16), VMEM((taps, value_rows), F32),
            VMEM((groups, length), BF16), VMEM((taps, groups), F32), VMEM((groups, length), BF16), VMEM((taps, groups), F32),
            VMEM((heads, length), F32), VMEM((1, heads), F32), VMEM((value_rows, length), BF16), VMEM((1, value_rows), F32),
            VMEM((2 * hidden_units, features), BF16), VMEM((features, 2 * hidden_units), BF16), VMEM((hidden_units, features), BF16),
            VMEM((ep_size, tokens), F32), VMEM((ep_size, tokens), F32), VMEM((ep_size * pad, tokens), BF16),
            VMEM((ep_size, pad, width), BF16), VMEM((ep_size, pad, width), BF16),
            VMEM((tp_size, slots, width), BF16),
            VMEM((teams, 2, chips, span, width), BF16), VMEM((teams, chips, span, width), BF16),
            VMEM((2, teams, far, span, width), BF16), VMEM((2, teams, far, span, width), BF16),
            VMEM((ep_size, pad, width), BF16), VMEM((ep_size, pad, width), BF16),
            VMEM((RIM, value_rows + 2 * NSTATE), BF16), VMEM((RIM, value_rows + 2 * NSTATE), BF16),
            VMEM((value_rows, LANES), F32), VMEM((NSTATE, LANES), F32), VMEM((NSTATE, LANES), F32),
            VMEM((value_rows, taps), F32), VMEM((groups, taps), F32), VMEM((groups, taps), F32),
            VMEM((value_rows, LANES), F32),
            VMEM((heads, length), F32), VMEM((heads, length), F32), VMEM((heads, length, LANES), F32),
            VMEM((length, length), F32), VMEM((NSTATE, length), BF16), VMEM((NSTATE, length), BF16),
            VMEM((value_rows, length), BF16), VMEM((value_rows, length), F32),
            VMEM((heads, PACK, NSTATE), BF16), VMEM((ROWX, PACK, NSTATE), BF16),
            VMEM((PACK, NSTATE), BF16), VMEM((deep, PACK, NSTATE), BF16),
            VMEM((ROWX, HEAD_DIM, NSTATE), BF16), VMEM((ROWX, HEAD_DIM, NSTATE), BF16),
            VMEM((ROWX, HEAD_DIM, NSTATE), F32), VMEM((ROWX, 8, NSTATE), F32), VMEM((tokens, width), F32),
            dma((19,)), dma((1,)), dma((teams,)), dma((1,)), dma((1,)),
            dma((1,)), dma((teams, far)), dma((1,)), dma((teams,)),
            dma((1,)), dma((teams,)), dma((1,)), dma((teams, far - 1)),
            dma((1,)), dma((teams,)), dma((1,)), dma((1,)), dma((deep,)), dma((deep,)), dma((1,)), dma((1,)),
        ],
        compiler_params=pltpu.CompilerParams(collective_id=0, has_side_effects=True, vmem_limit_bytes=60 * 2**20),
        name="layer",
    )(
        moe_rows, moe_gain.reshape(1, features), routes.T, route_logit.T,
        x_in, conv_x.T, b_in, conv_b.T, c_in, conv_c.T, dt_raw, decay_rate.reshape(1, heads),
        z_in, head_gain.reshape(1, value_rows),
        jnp.swapaxes(w_gate, 1, 2), jnp.swapaxes(w_up, 1, 2), w_down,
    )
    mixed, moe = pl.pallas_call(
        emit_kernel,
        out_shape=(shape((value_rows, length), BF16), shape((tokens, width), BF16)),
        in_specs=vmem_specs(2),
        out_specs=tuple([pl.BlockSpec(memory_space=pltpu.HBM)] * 2),
        scratch_shapes=[dma((2,))],
        compiler_params=pltpu.CompilerParams(vmem_limit_bytes=8 * 2**20),
        name="emit",
    )(mixed, moe)
    return (mixed, moe.T)


def solution(mesh):
    return jax.shard_map(
        on_device,
        mesh=mesh,
        in_specs=(
            P("tp", "ep"), P("tp", "ep"), P("tp", "ep"), P("tp"), P(None, "ep"), P(None, "ep"),
            P("tp", None), P(), P(), P("tp"), P("ep", None), P(), P("ep", None), P("ep", None),
            P("ep", None, "tp"), P("ep", None, "tp"), P("ep", "tp", None),
        ),
        out_specs=(P("tp", "ep"), P("tp", "ep")),
        check_vma=False,
    )
```
